32 devices in a mesh: kv: 8 (over z, x), tp: 4 (over y, core).
Axes of the slice: x: 2, y: 2, z: 4, core: 2. Of those that a mesh axis runs over, the one named last changes fastest.
Arguments:
- tokens: bfloat16 [1024, 2048], P('kv', 'tp'), may hold values from -6 to 6
- states: float32 [1024, 16, 64, 64], P('kv', 'tp'), may hold values from -6 to 6
- mix_gain: bfloat16 [2048], replicated, may hold values from 0.099609375 to 1.8984375
- w_query: bfloat16 [2048, 1024], P(None, 'tp'), may hold values from -0.125 to 0.125
- w_key: bfloat16 [2048, 1024], P(None, 'tp'), may hold values from -0.125 to 0.125
- w_value: bfloat16 [2048, 1024], P(None, 'tp'), may hold values from -0.125 to 0.125
- w_gate: bfloat16 [2048, 1024], P(None, 'tp'), may hold values from -0.125 to 0.125
- head_gain: bfloat16 [1024], P('tp'), may hold values from 0.099609375 to 1.8984375
- w_output: bfloat16 [1024, 2048], P('tp'), may hold values from -0.1875 to 0.1875
- channel_gain: bfloat16 [2048], replicated, may hold values from 0.099609375 to 1.8984375
- w_up: bfloat16 [2048, 8192], P(None, 'kv'), may hold values from -0.125 to 0.125
- w_down: bfloat16 [8192, 2048], P('kv'), may hold values from -0.0625 to 0.0625
Outputs:
- layer_out: bfloat16 [1024, 2048], P('kv', 'tp')
- new_states: float32 [1024, 16, 64, 64], P('kv', 'tp')
The draws below stay inside these ranges and needn't reach their ends.
All inputs are finite; a program needn't handle non-finite values.
Results may differ from the reference program's by a relative error of at most 0.019.
Values may be sent and summed in bfloat16 or wider, within the bound.
A program may use at most 64 MiB of HBM per device.

```python
import jax
import jax.numpy as jnp
from jax import lax

D = 2048
HEADS = 16
HEAD = 64
FF = 8192
POS = 16384
BATCH = 1024
N_TP = 4


def draw_tokens(key, part):
    first_key = jax.random.fold_in(jax.random.fold_in(key, 11), 0)
    column = jnp.arange(D, dtype=jnp.float32) / D
    profile = 0.5 * jnp.exp(jnp.log(3.0) * column)
    drawn = jax.random.normal(first_key, (BATCH, D), jnp.float32) * profile
    return jnp.clip(drawn, -6.0, 6.0).astype(jnp.bfloat16)


def shard_levels(rng, extent, shards, smallest, high):
    gain = 1.0
    for dim, parts in shards:
        steps = jax.random.uniform(jax.random.fold_in(jax.random.fold_in(rng, 6), dim), (parts,), jnp.float32, smallest / len(shards), high / len(shards))
        gain = gain * jnp.repeat(jnp.exp(steps), extent[dim] // parts).reshape((-1,) + (1,) * (len(extent) - 1 - dim))
    return gain


def scatter_about(rng, extent, scale, bound, shards=(), kind=jnp.bfloat16):
    array = jax.random.normal(rng, extent, jnp.float32) * scale
    if len(shards) > 0:
        array = shard_levels(rng, extent, shards, -0.22, 0.18) * array
    return jnp.clip(array, min=-bound, max=bound).astype(kind)


def setup_inputs(seed: int = 0) -> dict:
    arg_keys = jax.random.split(jax.random.key(seed), 13)
    return {
        "tokens": draw_tokens(jax.random.fold_in(arg_keys[12], 71), 0),
        "states": scatter_about(arg_keys[1], (BATCH, HEADS, HEAD, HEAD), 1.0, 6.0, ((0, 8), (1, 4)), jnp.float32),
        "mix_gain": jnp.clip(1.0 + 0.18 * jax.random.normal(arg_keys[2], (D,), jnp.float32), 0.099609375, 1.8984375).astype(jnp.bfloat16),
        "w_query": scatter_about(arg_keys[3], (D, HEADS * HEAD), D ** -0.5, 0.125, ((1, 4),)),
        "w_key": scatter_about(arg_keys[4], (D, HEADS * HEAD), D ** -0.5, 0.125, ((1, 4),)),
        "w_value": scatter_about(arg_keys[5], (D, HEADS * HEAD), D ** -0.5, 0.125, ((1, 4),)),
        "w_gate": scatter_about(arg_keys[6], (D, HEADS * HEAD), D ** -0.5, 0.125, ((1, 4),)),
        "head_gain": jnp.clip(1.0 + 0.18 * jax.random.normal(arg_keys[7], (HEADS * HEAD,), jnp.float32), 0.099609375, 1.8984375).astype(jnp.bfloat16),
        "w_output": scatter_about(arg_keys[8], (HEADS * HEAD, D), (HEADS * HEAD) ** -0.5, 0.1875, ((0, 4),)),
        "channel_gain": jnp.clip(1.0 + 0.18 * jax.random.normal(arg_keys[9], (D,), jnp.float32), 0.099609375, 1.8984375).astype(jnp.bfloat16),
        "w_up": scatter_about(arg_keys[10], (D, FF), D ** -0.5, 0.125, ((1, 8),)),
        "w_down": scatter_about(arg_keys[11], (FF, D), FF ** -0.5, 0.0625, ((0, 8),)),
    }


EPSILON = 1e-06
ROTARY_BASE = 10000.0

def rotate(vectors):
    half_size = vectors.shape[-1] // 2
    frequency = ROTARY_BASE ** (-jnp.arange(half_size, dtype=jnp.float32) / half_size)
    angles = POS * frequency
    cosine = jnp.cos(angles)
    sines = jnp.sin(angles)
    first_half = vectors[..., :half_size]
    second = vectors[..., half_size:]
    return jnp.concatenate([first_half * cosine - second * sines, first_half * sines + second * cosine], axis=-1)

def retain(normed, states, w_query, w_key, w_value, w_gate, head_gain, head_ids):
    row_count = states.shape[0]
    head_count = states.shape[1]
    head_size = states.shape[2]

    def project(weight):
        return jnp.dot(normed, weight, preferred_element_type=jnp.float32).reshape(row_count, head_count, head_size)
    queries = rotate(project(w_query)) * head_size ** (-0.5)
    keys_now = rotate(project(w_key))
    values = project(w_value)
    gating = jnp.dot(normed, w_gate, preferred_element_type=jnp.float32)
    decays = 1.0 - jnp.exp2(-1.0 - 11.0 * head_ids / (HEADS - 1))
    new_states = decays[None, :, None, None] * states + keys_now[:, :, :, None] * values[:, :, None, :]
    output = jnp.einsum('bhk,bhkv->bhv', queries, new_states, precision=lax.Precision.HIGHEST)
    center = output - lax.optimization_barrier(jnp.mean(output, axis=-1, keepdims=True))
    spread = lax.optimization_barrier(jnp.mean(center * center, axis=-1, keepdims=True))
    scaled = center * lax.rsqrt(spread + EPSILON) * head_gain.astype(jnp.float32).reshape(head_count, head_size)
    gated_out = (scaled.reshape(row_count, head_count * head_size) * jax.nn.silu(gating)).astype(jnp.bfloat16)
    return (gated_out, new_states)

def reference(tokens, states, mix_gain, w_query, w_key, w_value, w_gate, head_gain, w_output, channel_gain, w_up, w_down):
    widened = tokens.astype(jnp.float32)
    inverse_rms = lax.rsqrt(lax.optimization_barrier(jnp.mean(widened * widened, axis=1, keepdims=True)) + EPSILON)
    normed = (widened * inverse_rms * mix_gain.astype(jnp.float32)).astype(jnp.bfloat16)
    head_ids = jnp.arange(HEADS).astype(jnp.float32)
    gated_out, new_states = retain(normed, states, w_query, w_key, w_value, w_gate, head_gain, head_ids)
    blocks = gated_out.astype(jnp.float32).reshape(BATCH, N_TP, -1)
    weights = w_output.astype(jnp.float32).reshape(N_TP, -1, D)
    partials = jnp.einsum('btc,tcd->btd', blocks, weights)
    rounded = lax.optimization_barrier(partials.astype(jnp.bfloat16))
    attended = lax.optimization_barrier(jnp.sum(rounded.astype(jnp.float32), axis=1))
    middle = (widened + attended).astype(jnp.bfloat16)
    mid_wide = middle.astype(jnp.float32)
    second_rms = lax.rsqrt(lax.optimization_barrier(jnp.mean(mid_wide * mid_wide, axis=1, keepdims=True)) + EPSILON)
    scaled = (mid_wide * channel_gain.astype(jnp.float32)).astype(jnp.bfloat16)
    hidden = jnp.dot(scaled, w_up, preferred_element_type=jnp.float32) * second_rms
    activated = jnp.square(jax.nn.relu(hidden)).astype(jnp.bfloat16)
    down_sum = jnp.dot(activated, w_down, preferred_element_type=jnp.float32)
    layer_out = (mid_wide + down_sum).astype(jnp.bfloat16)
    return (layer_out, new_states)
```

```python
import functools

import jax
import jax.numpy as jnp
import numpy as np
from jax import lax
from jax.experimental import pallas as pl
from jax.experimental.pallas import tpu as pltpu
from jax.sharding import PartitionSpec as P

POS = 16384
EPSILON = 1e-06
ROTARY_BASE = 10000.0
CORES = 2
PIECES = 2
SLICES = 4
MESH = pl.DeviceIdType.MESH
F32 = jnp.float32
BF16 = jnp.bfloat16


def dot(a, b):
    return jnp.dot(a, b, preferred_element_type=F32)


def kernel(
    sizes,
    tok_hbm, st_hbm, mix_hbm, wq_hbm, wk_hbm, wv_hbm, wg_hbm, head_hbm, wo_hbm,
    chan_hbm, wu_hbm, wd_hbm, turn_hbm,
    out_ref, st,
    mix_gain, chan_gain, head_gain, turn, gain1, gain2,
    xf, wproj, wo, wu, wd, acc, qt, kt, vt, rt,
    part, r1, s2, r2, mid, lhs, act, sx, rx, sz, rz, fin, ob,
    load_sem, a_send, a_recv, b1_send, b1_recv, b2_send, b2_recv,
    cx_send, cz_send, c_recv, dx_send, dx_recv, dz_send, dz_recv, e_send, e_recv,
):
    n_tp, ny, nz, nx, heads, head, rows, feats, share, width, parts = sizes
    tp = lax.axis_index("tp")
    kv = lax.axis_index("kv")
    c, y = lax.rem(tp, CORES), tp // CORES
    x, z = lax.rem(kv, nx), kv // nx
    other = 1 - c
    partner = y * CORES + other
    half = head // 2
    piece = width // PIECES
    strip = width // SLICES
    few = share // parts

    def ys(d):
        return lax.rem(y + d, ny)

    def zs(d):
        return lax.rem(z + d, nz)

    def xs(d):
        return lax.rem(x + d, nx)

    def make(src, dst, ssem, rsem, device):
        return pltpu.make_async_remote_copy(
            src_ref=src, dst_ref=dst, send_sem=ssem, recv_sem=rsem,
            device_id=device, device_id_type=MESH,
        )

    early, late = [], []

    def send(src, dst, ssem, rsem, device, log):
        copy = make(src, dst, ssem, rsem, device)
        copy.start()
        log.append((None, copy))

    def send_if(cond, src, dst, ssem, rsem, device, log):
        copy = make(src, dst, ssem, rsem, device)
        pl.when(cond)(copy.start)
        log.append((cond, copy))

    def drain(log):
        for cond, copy in log:
            if cond is None:
                copy.wait_send()
            else:
                pl.when(cond)(copy.wait_send)
        log.clear()

    def arrive(dst, ssem, rsem, device):
        make(dst, dst, ssem, rsem, device).wait_recv()

    barrier = pltpu.get_barrier_semaphore()
    greeted = 0
    for d in range(1, n_tp):
        pl.semaphore_signal(barrier, inc=1, device_id={"tp": lax.rem(tp + d, n_tp)}, device_id_type=MESH)
        greeted += 1
    for d in range(1, nx):
        pl.semaphore_signal(barrier, inc=1, device_id={"kv": z * nx + xs(d)}, device_id_type=MESH)
        greeted += 1
    for d in range(1, nz):
        pl.semaphore_signal(barrier, inc=1, device_id={"kv": zs(d) * nx + x}, device_id_type=MESH)
        greeted += 1

    slots = iter(range(12 + heads))

    def load(src, dst):
        copy = pltpu.make_async_copy(src, dst, load_sem.at[next(slots)])
        copy.start()
        return copy

    tok_load = load(tok_hbm, xf.at[tp])
    mix_load = load(mix_hbm, mix_gain)
    proj_loads = [load(w, wproj.at[i]) for i, w in enumerate((wq_hbm, wk_hbm, wv_hbm, wg_hbm))]
    turn_load = load(turn_hbm, turn)
    st_loads = [load(st_hbm.at[h], st.at[h]) for h in range(heads)]
    head_load = load(head_hbm, head_gain)
    wo_load = load(wo_hbm, wo)
    chan_load = load(chan_hbm, chan_gain)
    wu_load = load(wu_hbm, wu)
    wd_load = load(wd_hbm, wd)
    tok_load.wait()
    pl.semaphore_wait(barrier, greeted)

    for d in range(1, ny):
        send(xf.at[tp], xf.at[tp], a_send.at[d], a_recv.at[tp], {"tp": ys(d) * CORES + c}, early)
    send(xf.at[tp], xf.at[tp], a_send.at[0], a_recv.at[tp], {"tp": partner}, early)
    mix_load.wait()
    gain1[...] = mix_gain[...].astype(F32).reshape(1, width)

    squares = jnp.zeros((rows, 1), F32)

    def project(slot, first, squares):
        at = pl.ds(pl.multiple_of(slot * feats, feats), feats)
        wide = xf[slot].astype(F32)
        scaled = (wide * gain1[:, at]).astype(BF16)
        for i in range(4):
            if first:
                proj_loads[i].wait()
            term = dot(scaled, wproj[i, at, :])
            if first:
                acc[i] = term
            else:
                acc[i] += term
        return squares + jnp.sum(wide * wide, axis=1, keepdims=True)

    squares = project(tp, True, squares)
    arrive(xf.at[partner], a_send.at[0], a_recv.at[partner], {"tp": partner})
    squares = project(partner, False, squares)
    for d in range(1, ny):
        slot = ys(d) * CORES + c
        arrive(xf.at[slot], a_send.at[0], a_recv.at[slot], {"tp": slot})
        send(xf.at[slot], xf.at[slot], a_send.at[ny + d], a_recv.at[slot], {"tp": partner}, early)
        squares = project(slot, False, squares)
        slot = ys(d) * CORES + other
        arrive(xf.at[slot], a_send.at[0], a_recv.at[slot], {"tp": partner})
        squares = project(slot, False, squares)
    inverse = lax.rsqrt(squares * (1.0 / width) + EPSILON)

    qt[...] = (acc[0] * inverse).T
    kt[...] = (acc[1] * inverse).T
    vt[...] = (acc[2] * inverse).T
    turn_load.wait()
    cosine, sine = turn[:half, :], turn[half:, :]
    for h in range(heads):
        lo, hi = pl.ds(h * head, half), pl.ds(h * head + half, half)
        for ref, scale in ((qt, head ** -0.5), (kt, 1.0)):
            a, b = ref[lo, :], ref[hi, :]
            ref[lo, :] = (a * cosine - b * sine) * scale
            ref[hi, :] = (a * sine + b * cosine) * scale
    for h in range(heads):
        st_loads[h].wait()
        number = (tp * heads + h).astype(F32)
        decay = 1.0 - jnp.exp2(-1.0 - 11.0 * jnp.full((1, rows), number, F32) / (heads * n_tp - 1))
        value = vt[pl.ds(h * head, head), :]
        base = h * head

        def step(k, total, h=h, base=base, decay=decay, value=value):
            fresh = decay * st[h, k] + kt[pl.ds(base + k, 1), :] * value
            st[h, k] = fresh
            return total + qt[pl.ds(base + k, 1), :] * fresh

        total = lax.fori_loop(0, head, step, jnp.zeros((head, rows), F32), unroll=8)
        center = total - jnp.mean(total, axis=0, keepdims=True)
        spread = jnp.mean(center * center, axis=0, keepdims=True)
        rt[pl.ds(base, head), :] = center * lax.rsqrt(spread + EPSILON)
    gating = acc[3] * inverse
    head_load.wait()
    gated = (rt[...].T * head_gain[...].astype(F32).reshape(1, heads * head) * (gating * jax.nn.sigmoid(gating))).astype(BF16)

    wo_load.wait()
    for j in range(PIECES):
        whole = dot(gated, wo[:, j * piece:(j + 1) * piece]).astype(BF16)
        for t in range(n_tp):
            for k in range(parts):
                part[k, j, t % CORES, t // CORES] = whole[t * share + k * few:t * share + (k + 1) * few]
        for k in range(parts):
            send(part.at[k, j, other], r1.at[k, j], b1_send.at[k, j], b1_recv.at[k, j], {"tp": partner}, early)

    for k in range(parts):
        for j in range(PIECES):
            arrive(r1.at[k, j], b1_send.at[0, 0], b1_recv.at[k, j], {"tp": partner})
            for d in range(1, ny):
                to = ys(d)
                s2[k, j, to] = (part[k, j, c, to].astype(F32) + r1[k, j, to].astype(F32)).astype(BF16)
                send(s2.at[k, j, to], r2.at[k, j, y], b2_send.at[k, j, d], b2_recv.at[k, j, y], {"tp": to * CORES + c}, early)
    chan_load.wait()
    gain2[...] = chan_gain[...].astype(F32).reshape(1, width)

    below, above = z > 0, z < nz - 1
    for k in range(parts):
        own_rows = pl.ds(pl.multiple_of(tp * share + k * few, few), few)
        for j in range(PIECES):
            total = part[k, j, c, y].astype(F32) + r1[k, j, y].astype(F32)
            for d in range(1, ny):
                frm = ys(d)
                arrive(r2.at[k, j, frm], b2_send.at[0, 0, 0], b2_recv.at[k, j, frm], {"tp": frm * CORES + c})
                total += r2[k, j, frm].astype(F32)
            per = n_tp // PIECES
            mine = jnp.concatenate([xf[t, own_rows, :] for t in range(j * per, (j + 1) * per)], axis=1)
            mid[k, j, z, x] = (mine.astype(F32) + total).astype(BF16)
            block = mid.at[k, j, z, x]
            send_if(above, block, block, cz_send.at[k, j, 0], c_recv.at[k, j, z, x], {"kv": (z + 1) * nx + x}, late)
            send_if(below, block, block, cz_send.at[k, j, nz], c_recv.at[k, j, z, x], {"kv": (z - 1) * nx + x}, late)
            for d in range(1, nx):
                send(block, block, cx_send.at[k, j, 0, d], c_recv.at[k, j, z, x], {"kv": z * nx + xs(d)}, late)

    room = jnp.minimum(z, nz - 1 - z)

    def near(s):
        step = jnp.where(s <= 2 * room, (s + 1) // 2, s - room)
        up = jnp.where(s <= 2 * room, s % 2 == 1, z < nz - 1 - z)
        return jnp.where(up, z + step, z - step)

    order = [z] + [near(s) for s in range(1, nz)]

    def forward(k, s):
        g = order[s]
        up = g < z
        onward = jnp.where(up, z < nz - 1, z > 0)
        ahead = jnp.where(up, z + 1, z - 1)
        for j in range(PIECES):
            block = mid.at[k, j, g, x]
            arrive(block, cz_send.at[0, 0, 0], c_recv.at[k, j, g, x], {"kv": g * nx + x})
            send_if(onward, block, block, cz_send.at[k, j, s], c_recv.at[k, j, g, x], {"kv": ahead * nx + x}, late)
            for d in range(1, nx):
                send(block, block, cx_send.at[k, j, s, d], c_recv.at[k, j, g, x], {"kv": z * nx + xs(d)}, late)

    for s in range(1, nz):
        for k in range(parts):
            forward(k, s)
    drain(early)

    tall = nx * few
    total_rows = nz * tall
    hidden_units = wu.shape[1]
    up_tile = min(256, hidden_units)
    down_tile = min(256, strip)

    def gather(k):
        for s in range(nz):
            g = order[s]
            at = pl.ds(pl.multiple_of(g * tall, tall), tall)
            for j in range(PIECES):
                for d in range(1, nx):
                    xx = xs(d)
                    arrive(mid.at[k, j, g, xx], cz_send.at[0, 0, 0], c_recv.at[k, j, g, xx], {"kv": z * nx + xx})
                wide = mid[k, j, g].reshape(tall, piece).astype(F32)
                lhs[at, j * piece:(j + 1) * piece] = (wide * gain2[:, j * piece:(j + 1) * piece]).astype(BF16)
        sums = jnp.zeros((total_rows, 1), F32)
        for j in range(PIECES):
            wide = mid[k, j].reshape(total_rows, piece).astype(F32)
            sums += jnp.sum(wide * wide, axis=1, keepdims=True)
        return lax.rsqrt(sums * (1.0 / width) + EPSILON)

    def mixer(k):
        rms = gather(k)
        if k == 0:
            wu_load.wait()

        @pl.loop(0, hidden_units // up_tile)
        def _(i):
            at = pl.ds(pl.multiple_of(i * up_tile, up_tile), up_tile)
            hidden = jnp.maximum(dot(lhs[...], wu[:, at]) * rms, 0.0)
            act[:, at] = (hidden * hidden).astype(BF16)

        if k == 0:
            wd_load.wait()

        for q in range(SLICES):
            for i in range(strip // down_tile):
                low = q * strip + i * down_tile
                down = dot(act[...], wd[:, low:low + down_tile]).astype(BF16)
                for zz in range(nz):
                    for xx in range(nx):
                        first = (zz * nx + xx) * few
                        sx[k, q, xx, zz, :, i * down_tile:(i + 1) * down_tile] = down[first:first + few]
            for d in range(1, nx):
                xx = xs(d)
                send(sx.at[k, q, xx], rx.at[k, q, x], dx_send.at[k, q, d], dx_recv.at[k, q, x], {"kv": z * nx + xx}, late)

    def reduce_x(k, q):
        for d in range(1, nx):
            xx = xs(d)
            arrive(rx.at[k, q, xx], dx_send.at[0, 0, 0], dx_recv.at[k, q, xx], {"kv": z * nx + xx})
        for s in range(nz - 1, 0, -1):
            g = order[s]
            total = sx[k, q, x, g].astype(F32)
            for d in range(1, nx):
                total += rx[k, q, xs(d), g].astype(F32)
            sz[k, q, g] = total.astype(BF16)
            send(sz.at[k, q, g], rz.at[k, q, z], dz_send.at[k, q, s], dz_recv.at[k, q, z], {"kv": g * nx + x}, late)

    for k in range(parts):
        mixer(k)
    for k in range(parts):
        for q in range(SLICES):
            reduce_x(k, q)

    per_piece, per_strip = piece // strip, strip // feats
    for k in range(parts):
        for q in range(SLICES):
            inside = q % per_piece
            total = sx[k, q, x, z].astype(F32)
            for d in range(1, nx):
                total += rx[k, q, xs(d), z].astype(F32)
            total += mid[k, q // per_piece, z, x, :, inside * strip:(inside + 1) * strip].astype(F32)
            for s in range(1, nz):
                g = order[s]
                arrive(rz.at[k, q, g], dz_send.at[0, 0, 0], dz_recv.at[k, q, g], {"kv": g * nx + x})
                total += rz[k, q, g].astype(F32)
            done = total.astype(BF16)
            for i in range(per_strip):
                t = q * per_strip + i
                fin[k, t] = done[:, i * feats:(i + 1) * feats]

                @pl.when(tp != t)
                def _(t=t, k=k):
                    make(fin.at[k, t], ob.at[tp, k], e_send.at[k, t], e_recv.at[k, tp], {"tp": t}).start()

                @pl.when(tp == t)
                def _(t=t, k=k):
                    ob[tp, k] = fin[k, t]

    drain(late)
    for k in range(parts):
        for d in range(1, n_tp):
            frm = lax.rem(tp + d, n_tp)
            arrive(ob.at[frm, k], e_send.at[0, 0], e_recv.at[k, frm], {"tp": frm})
            make(fin.at[k, frm], ob.at[tp, k], e_send.at[k, frm], e_recv.at[k, tp], {"tp": frm}).wait_send()
    out_ref[...] = ob[...].reshape(rows, feats)


def publish(out_ref, st, out_hbm, st_hbm, sem):
    heads, head = st.shape[0], st.shape[1]
    cuts = 2
    copies = []
    for h in range(heads):
        for i in range(cuts):
            at = pl.ds(i * (head // cuts), head // cuts)
            copies.append(pltpu.make_async_copy(st.at[h, at], st_hbm.at[h, at], sem.at[1 + h * cuts + i]))
    copies.append(pltpu.make_async_copy(out_ref, out_hbm, sem.at[0]))
    for copy in copies:
        copy.start()
    for copy in copies:
        copy.wait()


def local(
    n_kv, n_tp,
    tokens, states, mix_gain, w_query, w_key, w_value, w_gate, head_gain, w_output,
    channel_gain, w_up, w_down,
):
    rows, feats = tokens.shape
    heads, head = states.shape[1], states.shape[2]
    width = mix_gain.shape[0]
    inner = w_query.shape[1]
    hidden = w_up.shape[1]
    share = rows // n_tp
    nx = 1
    while (2 * nx) ** 2 <= n_kv:
        nx *= 2
    nz = n_kv // nx
    ny = n_tp // CORES
    piece = width // PIECES
    strip = width // SLICES
    parts = 2 if share % 32 == 0 else 1
    few = share // parts
    angles = POS * ROTARY_BASE ** (-np.arange(head // 2) / (head // 2))
    turn = np.concatenate([np.cos(angles), np.sin(angles)])[:, None]
    turn = jnp.asarray(np.broadcast_to(turn, (head, rows)), F32)
    sizes = (n_tp, ny, nz, nx, heads, head, rows, feats, share, width, parts)
    hbm = pl.BlockSpec(memory_space=pltpu.HBM)
    vmem = pl.BlockSpec(memory_space=pltpu.VMEM)
    dma = pltpu.SemaphoreType.DMA
    layer_out, new_states = pl.pallas_call(
        functools.partial(kernel, sizes),
        out_shape=(
            pltpu.VMEM((rows, feats), BF16),
            pltpu.VMEM((heads, head, head, rows), F32),
        ),
        in_specs=[hbm] * 13,
        out_specs=(vmem, vmem),
        scratch_shapes=[
            pltpu.VMEM((width,), BF16),
            pltpu.VMEM((width,), BF16),
            pltpu.VMEM((inner,), BF16),
            pltpu.VMEM((head, rows), F32),
            pltpu.VMEM((1, width), F32),
            pltpu.VMEM((1, width), F32),
            pltpu.VMEM((n_tp, rows, feats), BF16),
            pltpu.VMEM((4, width, inner), BF16),
            pltpu.VMEM((inner, width), BF16),
            pltpu.VMEM((width, hidden), BF16),
            pltpu.VMEM((hidden, width), BF16),
            pltpu.VMEM((4, rows, inner), F32),
            pltpu.VMEM((inner, rows), F32),
            pltpu.VMEM((inner, rows), F32),
            pltpu.VMEM((inner, rows), F32),
            pltpu.VMEM((inner, rows), F32),
            pltpu.VMEM((parts, PIECES, CORES, ny, few, piece), BF16),
            pltpu.VMEM((parts, PIECES, ny, few, piece), BF16),
            pltpu.VMEM((parts, PIECES, ny, few, piece), BF16),
            pltpu.VMEM((parts, PIECES, ny, few, piece), BF16),
            pltpu.VMEM((parts, PIECES, nz, nx, few, piece), BF16),
            pltpu.VMEM((nz * nx * few, width), BF16),
            pltpu.VMEM((nz * nx * few, hidden), BF16),
            pltpu.VMEM((parts, SLICES, nx, nz, few, strip), BF16),
            pltpu.VMEM((parts, SLICES, nx, nz, few, strip), BF16),
            pltpu.VMEM((parts, SLICES, nz, few, strip), BF16),
            pltpu.VMEM((parts, SLICES, nz, few, strip), BF16),
            pltpu.VMEM((parts, n_tp, few, feats), BF16),
            pltpu.VMEM((n_tp, parts, few, feats), BF16),
            dma((12 + heads,)),
            dma((2 * ny,)),
            dma((n_tp,)),
            dma((parts, PIECES)),
            dma((parts, PIECES)),
            dma((parts, PIECES, ny)),
            dma((parts, PIECES, ny)),
            dma((parts, PIECES, nz, nx)),
            dma((parts, PIECES, nz + 1)),
            dma((parts, PIECES, nz, nx)),
            dma((parts, SLICES, nx)),
            dma((parts, SLICES, nx)),
            dma((parts, SLICES, nz)),
            dma((parts, SLICES, nz)),
            dma((parts, n_tp)),
            dma((parts, n_tp)),
        ],
        compiler_params=pltpu.CompilerParams(
            collective_id=0, has_side_effects=True, vmem_limit_bytes=48 * 1024 * 1024
        ),
    )(
        tokens, jnp.transpose(states, (1, 2, 3, 0)), mix_gain, w_query, w_key, w_value,
        w_gate, head_gain, w_output, channel_gain, w_up, w_down, turn,
    )
    layer_out, new_states = pl.pallas_call(
        publish,
        out_shape=(
            jax.ShapeDtypeStruct((rows, feats), BF16),
            jax.ShapeDtypeStruct((heads, head, head, rows), F32),
        ),
        in_specs=[vmem, vmem],
        out_specs=(hbm, hbm),
        scratch_shapes=[dma((1 + 2 * heads,))],
        compiler_params=pltpu.CompilerParams(vmem_limit_bytes=1024 * 1024),
    )(
        pltpu.with_memory_space_constraint(layer_out, pltpu.VMEM),
        pltpu.with_memory_space_constraint(new_states, pltpu.VMEM),
    )
    return (layer_out, jnp.transpose(new_states, (3, 0, 1, 2)))


def solution(mesh):
    placed = (
        P("kv", "tp"),
        P("kv", "tp", None, None),
        P(),
        P(None, "tp"),
        P(None, "tp"),
        P(None, "tp"),
        P(None, "tp"),
        P("tp"),
        P("tp", None),
        P(),
        P(None, "kv"),
        P("kv", None),
    )
    return jax.shard_map(
        functools.partial(local, mesh.shape["kv"], mesh.shape["tp"]),
        mesh=mesh,
        in_specs=placed,
        out_specs=(P("kv", "tp"), P("kv", "tp", None, None)),
        check_vma=False,
    )
```

```python
import functools

import jax
import jax.numpy as jnp
import numpy as np
from jax import lax
from jax.experimental import pallas as pl
from jax.experimental.pallas import tpu as pltpu
from jax.sharding import PartitionSpec as P

POS = 16384
EPSILON = 1e-06
ROTARY_BASE = 10000.0
CORES = 2
CUTS = 2
PIECES = 4
CROSS = 0
SLICES = 4
MESH = pl.DeviceIdType.MESH
F32 = jnp.float32
BF16 = jnp.bfloat16


def dot(a, b):
    return jnp.dot(a, b, preferred_element_type=F32)


def kernel(
    sizes,
    tok_hbm, st_hbm, mix_hbm, wq_hbm, wk_hbm, wv_hbm, wg_hbm, head_hbm, wo_hbm,
    chan_hbm, wu_hbm, wd_hbm, turn_hbm,
    out_ref, st,
    mix_gain, chan_gain, head_gain, turn, gain1, gain2,
    xf, wproj, wo, wu, wd, acc, qt, kt, vt, rt,
    part, r1, s2, r2, mid, lhs, act, sx, rx, own, sz, rz, fin, ob,
    load_sem, a_send, a_recv, b1_send, b1_recv, b2_send, b2_recv,
    cx_send, cz_send, line_recv, cross_recv, side_recv,
    dx_send, dx_recv, own_recv, dz_send, dz_recv, e_send, e_recv,
):
    n_tp, ny, nz, nx, heads, head, rows, feats, share, width, parts = sizes
    tp = lax.axis_index("tp")
    kv = lax.axis_index("kv")
    c, y = lax.rem(tp, CORES), tp // CORES
    x, z = lax.rem(kv, nx), kv // nx
    other = 1 - c
    partner = y * CORES + other
    half = head // 2
    cut = width // CUTS
    piece = width // PIECES
    strip = width // SLICES
    few = share // parts

    def ys(d):
        return lax.rem(y + d, ny)

    def zs(d):
        return lax.rem(z + d, nz)

    def xs(d):
        return lax.rem(x + d, nx)

    def make(src, dst, ssem, rsem, device):
        return pltpu.make_async_remote_copy(
            src_ref=src, dst_ref=dst, send_sem=ssem, recv_sem=rsem,
            device_id=device, device_id_type=MESH,
        )

    def send(src, dst, ssem, rsem, device):
        make(src, dst, ssem, rsem, device).start()

    def send_if(cond, src, dst, ssem, rsem, device):
        pl.when(cond)(make(src, dst, ssem, rsem, device).start)

    def arrive(dst, rsem):
        make(dst, dst, a_send.at[0], rsem, {"tp": partner}).wait_recv()

    def sent(src, ssem):
        make(src, src, ssem, a_recv.at[0], {"tp": partner}).wait_send()

    barrier = pltpu.get_barrier_semaphore()
    greeted = 0
    for d in range(1, n_tp):
        pl.semaphore_signal(barrier, inc=1, device_id={"tp": lax.rem(tp + d, n_tp)}, device_id_type=MESH)
        greeted += 1
    for d in range(1, nx):
        pl.semaphore_signal(barrier, inc=1, device_id={"kv": z * nx + xs(d)}, device_id_type=MESH)
        greeted += 1
    for d in range(1, nz):
        pl.semaphore_signal(barrier, inc=1, device_id={"kv": zs(d) * nx + x}, device_id_type=MESH)
        greeted += 1

    slots = iter(range(9 + heads))

    def load(src, dst, slot=None):
        copy = pltpu.make_async_copy(src, dst, load_sem.at[next(slots) if slot is None else slot])
        copy.start()
        return copy

    tok_load = load(tok_hbm, xf.at[tp])
    mix_load = load(mix_hbm, mix_gain)
    shared = next(slots)
    for i, w in enumerate((wq_hbm, wk_hbm, wv_hbm, wg_hbm)):
        load(w, wproj.at[i], shared)
    turn_load = load(turn_hbm, turn)
    st_loads = [load(st_hbm.at[h], st.at[h]) for h in range(heads)]
    head_load = load(head_hbm, head_gain)
    wo_load = load(wo_hbm, wo)
    chan_load = load(chan_hbm, chan_gain)
    wu_load = load(wu_hbm, wu)
    wd_load = load(wd_hbm, wd)
    tok_load.wait()
    pl.semaphore_wait(barrier, greeted)

    for d in range(1, ny):
        send(xf.at[tp], xf.at[tp], a_send.at[0], a_recv.at[tp], {"tp": ys(d) * CORES + c})
    send(xf.at[tp], xf.at[tp], a_send.at[0], a_recv.at[tp], {"tp": partner})
    mix_load.wait()
    gain1[...] = mix_gain[...].astype(F32).reshape(1, width)

    squares = jnp.zeros((rows, 1), F32)

    def project(slot, first, squares):
        at = pl.ds(pl.multiple_of(slot * feats, feats), feats)
        wide = xf[slot].astype(F32)
        scaled = (wide * gain1[:, at]).astype(BF16)
        for i in range(4):
            term = dot(scaled, wproj[i, at, :])
            if first:
                acc[i] = term
            else:
                acc[i] += term
        return squares + jnp.sum(wide * wide, axis=1, keepdims=True)

    pltpu.make_async_copy(wproj, wproj, load_sem.at[shared]).wait()
    squares = project(tp, True, squares)
    arrive(xf.at[partner], a_recv.at[partner])
    squares = project(partner, False, squares)
    for d in range(1, ny):
        slot = ys(d) * CORES + c
        arrive(xf.at[slot], a_recv.at[slot])
        send(xf.at[slot], xf.at[slot], a_send.at[0], a_recv.at[slot], {"tp": partner})
        squares = project(slot, False, squares)
        slot = ys(d) * CORES + other
        arrive(xf.at[slot], a_recv.at[slot])
        squares = project(slot, False, squares)
    inverse = lax.rsqrt(squares * (1.0 / width) + EPSILON)

    qt[...] = (acc[0] * inverse).T
    kt[...] = (acc[1] * inverse).T
    vt[...] = (acc[2] * inverse).T
    turn_load.wait()
    cosine, sine = turn[:half, :], turn[half:, :]
    for h in range(heads):
        lo, hi = pl.ds(h * head, half), pl.ds(h * head + half, half)
        for ref, scale in ((qt, head ** -0.5), (kt, 1.0)):
            a, b = ref[lo, :], ref[hi, :]
            ref[lo, :] = (a * cosine - b * sine) * scale
            ref[hi, :] = (a * sine + b * cosine) * scale
    for h in range(heads):
        st_loads[h].wait()
        number = (tp * heads + h).astype(F32)
        decay = 1.0 - jnp.exp2(-1.0 - 11.0 * jnp.full((1, rows), number, F32) / (heads * n_tp - 1))
        value = vt[pl.ds(h * head, head), :]
        base = h * head

        def step(k, total, h=h, base=base, decay=decay, value=value):
            fresh = decay * st[h, k] + kt[pl.ds(base + k, 1), :] * value
            st[h, k] = fresh
            return total + qt[pl.ds(base + k, 1), :] * fresh

        total = lax.fori_loop(0, head, step, jnp.zeros((head, rows), F32), unroll=8)
        center = total - jnp.mean(total, axis=0, keepdims=True)
        spread = jnp.mean(center * center, axis=0, keepdims=True)
        rt[pl.ds(base, head), :] = center * lax.rsqrt(spread + EPSILON)
    gating = acc[3] * inverse
    head_load.wait()
    gated = (rt[...].T * head_gain[...].astype(F32).reshape(1, heads * head) * (gating * jax.nn.sigmoid(gating))).astype(BF16)

    wo_load.wait()
    for j in range(CUTS):
        whole = dot(gated, wo[:, j * cut:(j + 1) * cut]).astype(BF16)
        for t in range(n_tp):
            for k in range(parts):
                part[k, j, t % CORES, t // CORES] = whole[t * share + k * few:t * share + (k + 1) * few]
        for k in range(parts):
            send(part.at[k, j, other], r1.at[k, j], b1_send.at[0], b1_recv.at[k, j], {"tp": partner})

    for k in range(parts):
        for j in range(CUTS):
            arrive(r1.at[k, j], b1_recv.at[k, j])
            for d in range(1, ny):
                to = ys(d)
                s2[k, j, d - 1] = (part[k, j, c, to].astype(F32) + r1[k, j, to].astype(F32)).astype(BF16)
                send(s2.at[k, j, d - 1], r2.at[k, j, d - 1], b2_send.at[0], b2_recv.at[k, j, d - 1], {"tp": to * CORES + c})
    chan_load.wait()
    gain2[...] = chan_gain[...].astype(F32).reshape(1, width)

    below, above = z > 0, z < nz - 1

    def along(block, recv, up_sem, down_sem):
        send_if(above, block, block, up_sem, recv, {"kv": (z + 1) * nx + x})
        send_if(below, block, block, down_sem, recv, {"kv": (z - 1) * nx + x})

    def across(block, sem, recv):
        for d in range(1, nx):
            send(block, block, sem, recv(nx - 1 - d), {"kv": z * nx + xs(d)})

    for k in range(parts):
        own_rows = pl.ds(pl.multiple_of(tp * share + k * few, few), few)
        for b in range(CUTS):
            total = part[k, b, c, y].astype(F32) + r1[k, b, y].astype(F32)
            for d in range(1, ny):
                arrive(r2.at[k, b, d - 1], b2_recv.at[k, b, d - 1])
                total += r2[k, b, d - 1].astype(F32)
            per = n_tp // CUTS
            mine = jnp.concatenate([xf[t, own_rows, :] for t in range(b * per, (b + 1) * per)], axis=1)
            middle = (mine.astype(F32) + total).astype(BF16)
            for i in range(cut // piece):
                j = b * (cut // piece) + i
                mid[k, j, z, x] = middle[:, i * piece:(i + 1) * piece]
                block = mid.at[k, j, z, x]
                if j < CROSS:
                    across(block, cx_send.at[0], lambda r, k=k, j=j: cross_recv.at[k, j, z, r])
                    along(block, line_recv.at[k, j, z], cz_send.at[0], cz_send.at[1])
                else:
                    along(block, line_recv.at[k, j, z], cz_send.at[0], cz_send.at[1])
                    across(block, cx_send.at[0], lambda r, k=k: side_recv.at[k, z, r])

    room = jnp.minimum(z, nz - 1 - z)

    def near(s):
        step = jnp.where(s <= 2 * room, (s + 1) // 2, s - room)
        up = jnp.where(s <= 2 * room, s % 2 == 1, z < nz - 1 - z)
        return jnp.where(up, z + step, z - step)

    order = [z] + [near(s) for s in range(1, nz)]

    def cross(k):
        for j in range(CROSS):
            for d in range(1, nx):
                block = mid.at[k, j, z, xs(d)]
                recv = cross_recv.at[k, j, z, d - 1]
                arrive(block, recv)
                along(block, recv, cz_send.at[2], cz_send.at[3])

    def forward(k, s):
        g = order[s]
        up = g < z
        onward = jnp.where(up, z < nz - 1, z > 0)
        device = {"kv": jnp.where(up, z + 1, z - 1) * nx + x}
        for j in range(PIECES):
            block, recv = mid.at[k, j, g, x], line_recv.at[k, j, g]
            arrive(block, recv)
            send_if(onward, block, block, cz_send.at[2 + 2 * s], recv, device)
            if j < CROSS:
                for d in range(1, nx):
                    block, recv = mid.at[k, j, g, xs(d)], cross_recv.at[k, j, g, d - 1]
                    arrive(block, recv)
                    send_if(onward, block, block, cz_send.at[3 + 2 * s], recv, device)
            else:
                across(block, cx_send.at[1], lambda r, k=k, g=g: side_recv.at[k, g, r])

    def drain_gather():
        sent(mid.at[:, :, 0, 0:nx - 1], cx_send.at[0])
        sent(mid.at[:, 0:PIECES - CROSS, 0:nz - 1, 0:nx - 1], cx_send.at[1])
        straight = mid.at[:, :, 0, 0]
        crossed = mid.at[:, 0:max(CROSS, 1), 0, 0:nx - 1]
        for cond, first in ((above, 0), (below, 1)):
            pl.when(cond)(functools.partial(sent, straight, cz_send.at[first]))
            if CROSS:
                pl.when(cond)(functools.partial(sent, crossed, cz_send.at[2 + first]))
        for s in range(1, nz):
            onward = jnp.where(order[s] < z, z < nz - 1, z > 0)
            pl.when(onward)(functools.partial(sent, straight, cz_send.at[2 + 2 * s]))
            if CROSS:
                pl.when(onward)(functools.partial(sent, crossed, cz_send.at[3 + 2 * s]))

    for k in range(parts):
        cross(k)
    steps = [(k, s) for s in range(1, nz) for k in range(parts)]
    steps.sort(key=lambda e: (e[1] + 1.5 * e[0], e[0]))
    for k, s in steps:
        forward(k, s)
    sent(xf.at[0:2 * ny - 1], a_send.at[0])
    sent(r1, b1_send.at[0])
    sent(s2, b2_send.at[0])

    tall = nx * few
    total_rows = nz * tall
    hidden_units = wu.shape[1]
    up_tile = min(256, hidden_units)
    down_tile = min(256, strip)

    def gather(k):
        for s in range(nz):
            g = order[s]
            at = pl.ds(pl.multiple_of(g * tall, tall), tall)
            for d in range(1, nx):
                arrive(mid.at[k, 0:PIECES - CROSS, g, xs(d)], side_recv.at[k, g, d - 1])
            for j in range(PIECES):
                wide = mid[k, j, g].reshape(tall, piece).astype(F32)
                lhs[at, j * piece:(j + 1) * piece] = (wide * gain2[:, j * piece:(j + 1) * piece]).astype(BF16)
        sums = jnp.zeros((total_rows, 1), F32)
        for j in range(PIECES):
            wide = mid[k, j].reshape(total_rows, piece).astype(F32)
            sums += jnp.sum(wide * wide, axis=1, keepdims=True)
        return lax.rsqrt(sums * (1.0 / width) + EPSILON)

    def mixer(k):
        rms = gather(k)
        if k == 0:
            wu_load.wait()

        @pl.loop(0, hidden_units // up_tile)
        def _(i):
            at = pl.ds(pl.multiple_of(i * up_tile, up_tile), up_tile)
            hidden = jnp.maximum(dot(lhs[...], wu[:, at]) * rms, 0.0)
            act[:, at] = (hidden * hidden).astype(BF16)

        if k == 0:
            wd_load.wait()

        for q in range(SLICES):
            for i in range(strip // down_tile):
                low = q * strip + i * down_tile
                down = dot(act[...], wd[:, low:low + down_tile]).astype(BF16)
                for zz in range(nz):
                    for xx in range(nx):
                        first = (zz * nx + xx) * few
                        sx[k, xx, zz, q, :, i * down_tile:(i + 1) * down_tile] = down[first:first + few]
            for s in range(nz - 1, 0, -1):
                g = order[s]
                for d in range(1, nx):
                    send(sx.at[k, xs(d), g, q], rx.at[k, q, nx - 1 - d, g], dx_send.at[0], dx_recv.at[k, q], {"kv": z * nx + xs(d)})
            if k > 0:
                reduce_x(k - 1, q)

    def reduce_x(k, q):
        arrive(rx.at[k, q, :, 0:nz - 1], dx_recv.at[k, q])
        for s in range(nz - 1, 0, -1):
            g = order[s]
            total = sx[k, x, g, q].astype(F32)
            for d in range(1, nx):
                total += rx[k, q, d - 1, g].astype(F32)
            sz[k, q, g] = total.astype(BF16)
            send(sz.at[k, q, g], rz.at[k, q, z], dz_send.at[0], dz_recv.at[k, q], {"kv": g * nx + x})

    for k in range(parts):
        mixer(k)
    for k in range(parts):
        for d in range(1, nx):
            send(sx.at[k, xs(d), z], own.at[k, nx - 1 - d], dx_send.at[1], own_recv.at[k], {"kv": z * nx + xs(d)})
    drain_gather()
    for q in range(SLICES):
        reduce_x(parts - 1, q)

    per_strip = strip // feats
    per_piece = piece // strip if piece > strip else 1
    for k in range(parts):
        arrive(own.at[k], own_recv.at[k])
        for q in range(SLICES):
            inside = q % per_piece
            total = sx[k, x, z, q].astype(F32)
            for d in range(1, nx):
                total += own[k, d - 1, q].astype(F32)
            total += mid[k, q // per_piece, z, x, :, inside * strip:(inside + 1) * strip].astype(F32)
            arrive(rz.at[k, q, 0:nz - 1], dz_recv.at[k, q])
            for s in range(1, nz):
                total += rz[k, q, order[s]].astype(F32)
            done = total.astype(BF16)
            for i in range(per_strip):
                t = q * per_strip + i
                fin[k, t] = done[:, i * feats:(i + 1) * feats]

                @pl.when(tp != t)
                def _(t=t, k=k):
                    make(fin.at[k, t], ob.at[tp, k], e_send.at[0], e_recv.at[k], {"tp": t}).start()

                @pl.when(tp == t)
                def _(t=t, k=k):
                    ob[tp, k] = fin[k, t]

    sent(rx.at[:, :, :, 0:nz - 1], dx_send.at[0])
    sent(own, dx_send.at[1])
    sent(sz.at[:, :, 0:nz - 1], dz_send.at[0])
    for k in range(parts):
        arrive(ob.at[0:n_tp - 1, k], e_recv.at[k])
    sent(ob.at[0:n_tp - 1], e_send.at[0])
    out_ref[...] = ob[...].reshape(rows, feats)


def publish(out_ref, st, out_hbm, st_hbm, sem):
    heads, head = st.shape[0], st.shape[1]
    cuts = 2
    copies = []
    for h in range(heads):
        for i in range(cuts):
            at = pl.ds(i * (head // cuts), head // cuts)
            copies.append(pltpu.make_async_copy(st.at[h, at], st_hbm.at[h, at], sem.at[1 + h * cuts + i]))
    copies.append(pltpu.make_async_copy(out_ref, out_hbm, sem.at[0]))
    for copy in copies:
        copy.start()
    for copy in copies:
        copy.wait()


def local(
    n_kv, n_tp,
    tokens, states, mix_gain, w_query, w_key, w_value, w_gate, head_gain, w_output,
    channel_gain, w_up, w_down,
):
    rows, feats = tokens.shape
    heads, head = states.shape[1], states.shape[2]
    width = mix_gain.shape[0]
    inner = w_query.shape[1]
    hidden = w_up.shape[1]
    share = rows // n_tp
    nx = 1
    while (2 * nx) ** 2 <= n_kv:
        nx *= 2
    nz = n_kv // nx
    ny = n_tp // CORES
    cut = width // CUTS
    piece = width // PIECES
    strip = width // SLICES
    parts = 2 if share % 32 == 0 else 1
    few = share // parts
    angles = POS * ROTARY_BASE ** (-np.arange(head // 2) / (head // 2))
    turn = np.concatenate([np.cos(angles), np.sin(angles)])[:, None]
    turn = jnp.asarray(np.broadcast_to(turn, (head, rows)), F32)
    sizes = (n_tp, ny, nz, nx, heads, head, rows, feats, share, width, parts)
    hbm = pl.BlockSpec(memory_space=pltpu.HBM)
    vmem = pl.BlockSpec(memory_space=pltpu.VMEM)
    dma = pltpu.SemaphoreType.DMA
    layer_out, new_states = pl.pallas_call(
        functools.partial(kernel, sizes),
        out_shape=(
            pltpu.VMEM((rows, feats), BF16),
            pltpu.VMEM((heads, head, head, rows), F32),
        ),
        in_specs=[hbm] * 13,
        out_specs=(vmem, vmem),
        scratch_shapes=[
            pltpu.VMEM((width,), BF16),
            pltpu.VMEM((width,), BF16),
            pltpu.VMEM((inner,), BF16),
            pltpu.VMEM((head, rows), F32),
            pltpu.VMEM((1, width), F32),
            pltpu.VMEM((1, width), F32),
            pltpu.VMEM((n_tp, rows, feats), BF16),
            pltpu.VMEM((4, width, inner), BF16),
            pltpu.VMEM((inner, width), BF16),
            pltpu.VMEM((width, hidden), BF16),
            pltpu.VMEM((hidden, width), BF16),
            pltpu.VMEM((4, rows, inner), F32),
            pltpu.VMEM((inner, rows), F32),
            pltpu.VMEM((inner, rows), F32),
            pltpu.VMEM((inner, rows), F32),
            pltpu.VMEM((inner, rows), F32),
            pltpu.VMEM((parts, CUTS, CORES, ny, few, cut), BF16),
            pltpu.VMEM((parts, CUTS, ny, few, cut), BF16),
            pltpu.VMEM((parts, CUTS, ny - 1, few, cut), BF16),
            pltpu.VMEM((parts, CUTS, ny - 1, few, cut), BF16),
            pltpu.VMEM((parts, PIECES, nz, nx, few, piece), BF16),
            pltpu.VMEM((nz * nx * few, width), BF16),
            pltpu.VMEM((nz * nx * few, hidden), BF16),
            pltpu.VMEM((parts, nx, nz, SLICES, few, strip), BF16),
            pltpu.VMEM((parts, SLICES, nx - 1, nz, few, strip), BF16),
            pltpu.VMEM((parts, nx - 1, SLICES, few, strip), BF16),
            pltpu.VMEM((parts, SLICES, nz, few, strip), BF16),
            pltpu.VMEM((parts, SLICES, nz, few, strip), BF16),
            pltpu.VMEM((parts, n_tp, few, feats), BF16),
            pltpu.VMEM((n_tp, parts, few, feats), BF16),
            dma((9 + heads,)),
            dma((1,)),
            dma((n_tp,)),
            dma((1,)),
            dma((parts, CUTS)),
            dma((1,)),
            dma((parts, CUTS, ny - 1)),
            dma((2,)),
            dma((2 + 2 * nz,)),
            dma((parts, PIECES, nz)),
            dma((parts, max(CROSS, 1), nz, nx - 1)),
            dma((parts, nz, nx - 1)),
            dma((2,)),
            dma((parts, SLICES)),
            dma((parts,)),
            dma((1,)),
            dma((parts, SLICES)),
            dma((1,)),
            dma((parts,)),
        ],
        compiler_params=pltpu.CompilerParams(
            collective_id=0, has_side_effects=True, vmem_limit_bytes=48 * 1024 * 1024
        ),
    )(
        tokens, jnp.transpose(states, (1, 2, 3, 0)), mix_gain, w_query, w_key, w_value,
        w_gate, head_gain, w_output, channel_gain, w_up, w_down, turn,
    )
    layer_out, new_states = pl.pallas_call(
        publish,
        out_shape=(
            jax.ShapeDtypeStruct((rows, feats), BF16),
            jax.ShapeDtypeStruct((heads, head, head, rows), F32),
        ),
        in_specs=[vmem, vmem],
        out_specs=(hbm, hbm),
        scratch_shapes=[dma((1 + 2 * heads,))],
        compiler_params=pltpu.CompilerParams(vmem_limit_bytes=1024 * 1024),
    )(
        pltpu.with_memory_space_constraint(layer_out, pltpu.VMEM),
        pltpu.with_memory_space_constraint(new_states, pltpu.VMEM),
    )
    return (layer_out, jnp.transpose(new_states, (3, 0, 1, 2)))


def solution(mesh):
    placed = (
        P("kv", "tp"),
        P("kv", "tp", None, None),
        P(),
        P(None, "tp"),
        P(None, "tp"),
        P(None, "tp"),
        P(None, "tp"),
        P("tp"),
        P("tp", None),
        P(),
        P(None, "kv"),
        P("kv", None),
    )
    return jax.shard_map(
        functools.partial(local, mesh.shape["kv"], mesh.shape["tp"]),
        mesh=mesh,
        in_specs=placed,
        out_specs=(P("kv", "tp"), P("kv", "tp", None, None)),
        check_vma=False,
    )
```

```python
import functools

import jax
import jax.numpy as jnp
import numpy as np
from jax import lax
from jax.experimental import pallas as pl
from jax.experimental.pallas import tpu as pltpu
from jax.sharding import PartitionSpec as P

POS = 16384
EPSILON = 1e-06
ROTARY_BASE = 10000.0
CORES = 2
CUTS = 2
PIECES = 4
SLICES = 4
WAVES = 2
MESH = pl.DeviceIdType.MESH
F32 = jnp.float32
BF16 = jnp.bfloat16


def dot(a, b):
    return jnp.dot(a, b, preferred_element_type=F32)


def kernel(
    sizes,
    tok_hbm, st_hbm, mix_hbm, wq_hbm, wk_hbm, wv_hbm, wg_hbm, head_hbm, wo_hbm,
    chan_hbm, wu_hbm, wd_hbm, turn_hbm,
    out_ref, st,
    mix_gain, chan_gain, head_gain, turn, gain1, gain2,
    xf, wproj, wo, wu, wd, acc, qt, kt, vt, rt,
    part, r1, s2, r2, mid, lhs, act, sx, rx, own, sz, rz, fin, ob,
    load_sem, a_send, a_recv, b1_send, b1_recv, b2_send, b2_recv,
    cx_send, cz_send, line_recv, side_recv,
    dx_send, dx_recv, own_recv, dz_send, dz_recv, e_send, e_recv,
):
    n_tp, ny, nz, nx, heads, head, rows, feats, share, width, parts = sizes
    tp = lax.axis_index("tp")
    kv = lax.axis_index("kv")
    c, y = lax.rem(tp, CORES), tp // CORES
    x, z = lax.rem(kv, nx), kv // nx
    other = 1 - c
    partner = y * CORES + other
    half = head // 2
    cut = width // CUTS
    piece = width // PIECES
    strip = width // SLICES
    few = share // parts

    def ys(d):
        return lax.rem(y + d, ny)

    def zs(d):
        return lax.rem(z + d, nz)

    def xs(d):
        return lax.rem(x + d, nx)

    def make(src, dst, ssem, rsem, device):
        return pltpu.make_async_remote_copy(
            src_ref=src, dst_ref=dst, send_sem=ssem, recv_sem=rsem,
            device_id=device, device_id_type=MESH,
        )

    def send(src, dst, ssem, rsem, device):
        make(src, dst, ssem, rsem, device).start()

    def send_if(cond, src, dst, ssem, rsem, device):
        pl.when(cond)(make(src, dst, ssem, rsem, device).start)

    def arrive(dst, rsem):
        make(dst, dst, a_send.at[0], rsem, {"tp": partner}).wait_recv()

    def sent(src, ssem):
        make(src, src, ssem, a_recv.at[0, 0], {"tp": partner}).wait_send()

    barrier = pltpu.get_barrier_semaphore()
    greeted = 0
    for d in range(1, n_tp):
        pl.semaphore_signal(barrier, inc=1, device_id={"tp": lax.rem(tp + d, n_tp)}, device_id_type=MESH)
        greeted += 1
    for d in range(1, nx):
        pl.semaphore_signal(barrier, inc=1, device_id={"kv": z * nx + xs(d)}, device_id_type=MESH)
        greeted += 1
    for d in range(1, nz):
        pl.semaphore_signal(barrier, inc=1, device_id={"kv": zs(d) * nx + x}, device_id_type=MESH)
        greeted += 1

    slots = iter(range(7))

    def load(src, dst, slot=None):
        copy = pltpu.make_async_copy(src, dst, load_sem.at[next(slots) if slot is None else slot])
        copy.start()
        return copy

    tok_load = load(tok_hbm, xf.at[tp])
    small, shared, state = next(slots), next(slots), next(slots)
    load(mix_hbm, mix_gain, small)
    load(turn_hbm, turn, small)
    load(head_hbm, head_gain, small)
    load(chan_hbm, chan_gain, small)
    for i, w in enumerate((wq_hbm, wk_hbm, wv_hbm, wg_hbm)):
        load(w, wproj.at[i], shared)
    for h in range(heads):
        load(st_hbm.at[h], st.at[h], state)
    wo_load = load(wo_hbm, wo)
    wu_load = load(wu_hbm, wu)
    wd_load = load(wd_hbm, wd)
    tok_load.wait()
    pl.semaphore_wait(barrier, greeted)

    band = rows // parts

    def cutout(slot, k):
        return xf.at[slot, k * band:(k + 1) * band]

    for k in range(parts):
        for d in range(1, ny):
            send(cutout(tp, k), cutout(tp, k), a_send.at[0], a_recv.at[k, tp], {"tp": ys(d) * CORES + c})
        send(cutout(tp, k), cutout(tp, k), a_send.at[0], a_recv.at[k, tp], {"tp": partner})
    for ref in (mix_gain, turn, head_gain, chan_gain):
        pltpu.make_async_copy(ref, ref, load_sem.at[small]).wait()
    gain1[...] = mix_gain[...].astype(F32).reshape(1, width)
    pltpu.make_async_copy(wproj, wproj, load_sem.at[shared]).wait()

    def project(slot, low, count, first):
        at = pl.ds(pl.multiple_of(slot * feats, feats), feats)
        wide = xf[slot, low:low + count].astype(F32)
        scaled = (wide * gain1[:, at]).astype(BF16)
        for i in range(4):
            term = dot(scaled, wproj[i, at, :])
            if first:
                acc[i, low:low + count] = term
            else:
                acc[i, low:low + count] += term
        return jnp.sum(wide * wide, axis=1, keepdims=True)

    near_squares = project(tp, 0, rows, True)
    for k in range(parts):
        arrive(cutout(partner, k), a_recv.at[k, partner])
    near_squares += project(partner, 0, rows, False)

    def relay(k, d):
        slot = ys(d) * CORES + c
        arrive(cutout(slot, k), a_recv.at[k, slot])
        send(cutout(slot, k), cutout(slot, k), a_send.at[0], a_recv.at[k, slot], {"tp": partner})

    def finish(k, relayed):
        low = k * band
        squares = near_squares[low:low + band]
        for d in range(1, ny):
            if not relayed:
                relay(k, d)
            squares += project(ys(d) * CORES + c, low, band, False)
            slot = ys(d) * CORES + other
            arrive(cutout(slot, k), a_recv.at[k, slot])
            squares += project(slot, low, band, False)
        inverse = lax.rsqrt(squares * (1.0 / width) + EPSILON)

        def columns(i):
            value = acc[i, low:low + band] * inverse
            lead = [jnp.zeros((low, value.shape[1]), F32)] if low else []
            rest = [jnp.zeros((rows - low - band, value.shape[1]), F32)] if low + band < rows else []
            return jnp.concatenate(lead + [value] + rest, axis=0).T

        qt[...] = columns(0)
        kt[...] = columns(1)
        vt[...] = columns(2)
        cosine, sine = turn[:half, :], turn[half:, :]
        for h in range(heads):
            lo, hi = pl.ds(h * head, half), pl.ds(h * head + half, half)
            for ref, scale in ((qt, head ** -0.5), (kt, 1.0)):
                a, b = ref[lo, :], ref[hi, :]
                ref[lo, :] = (a * cosine - b * sine) * scale
                ref[hi, :] = (a * sine + b * cosine) * scale
        return inverse

    def retain(k, h):
        if k == 0 and h == 0:
            pltpu.make_async_copy(st, st, load_sem.at[state]).wait()
        number = (tp * heads + h).astype(F32)
        decay = 1.0 - jnp.exp2(-1.0 - 11.0 * jnp.full((1, rows), number, F32) / (heads * n_tp - 1))
        lane = lax.broadcasted_iota(jnp.int32, (1, rows), 1)
        decay = jnp.where((lane >= k * band) & (lane < (k + 1) * band), decay, 1.0)
        value = vt[pl.ds(h * head, head), :]
        base = h * head

        def step(i, total):
            fresh = decay * st[h, i] + kt[pl.ds(base + i, 1), :] * value
            st[h, i] = fresh
            return total + qt[pl.ds(base + i, 1), :] * fresh

        total = lax.fori_loop(0, head, step, jnp.zeros((head, rows), F32), unroll=8)
        center = total - jnp.mean(total, axis=0, keepdims=True)
        spread = jnp.mean(center * center, axis=0, keepdims=True)
        rt[pl.ds(base, head), :] = center * lax.rsqrt(spread + EPSILON)

    def output(k, inverse):
        low = k * band
        gating = acc[3, low:low + band] * inverse
        if k == 0:
            wo_load.wait()
        normal = rt[...].T[low:low + band]
        gated = (normal * head_gain[...].astype(F32).reshape(1, heads * head) * (gating * jax.nn.sigmoid(gating))).astype(BF16)
        for j in range(CUTS):
            whole = dot(gated, wo[:, j * cut:(j + 1) * cut]).astype(BF16)
            for t in range(n_tp):
                part[k, j, t % CORES, t // CORES] = whole[t * few:(t + 1) * few]
            send(part.at[k, j, other], r1.at[k, j], b1_send.at[0], b1_recv.at[k, j], {"tp": partner})

    def pairs(k):
        for j in range(CUTS):
            arrive(r1.at[k, j], b1_recv.at[k, j])
            for d in range(1, ny):
                to = ys(d)
                s2[k, j, d - 1] = (part[k, j, c, to].astype(F32) + r1[k, j, to].astype(F32)).astype(BF16)
                send(s2.at[k, j, d - 1], r2.at[k, j, d - 1], b2_send.at[0], b2_recv.at[k, j, d - 1], {"tp": to * CORES + c})

    below, above = z > 0, z < nz - 1

    def across(block, sem, recv):
        for d in range(1, nx):
            send(block, block, sem, recv.at[nx - 1 - d], {"kv": z * nx + xs(d)})

    def launch(k):
        own_rows = pl.ds(pl.multiple_of(k * band + tp * few, few), few)
        for b in range(CUTS):
            total = part[k, b, c, y].astype(F32) + r1[k, b, y].astype(F32)
            for d in range(1, ny):
                arrive(r2.at[k, b, d - 1], b2_recv.at[k, b, d - 1])
                total += r2[k, b, d - 1].astype(F32)
            per = n_tp // CUTS
            mine = jnp.concatenate([xf[t, own_rows, :] for t in range(b * per, (b + 1) * per)], axis=1)
            middle = (mine.astype(F32) + total).astype(BF16)
            for i in range(cut // piece):
                j = b * (cut // piece) + i
                mid[k, j, z, x] = middle[:, i * piece:(i + 1) * piece]
                block = mid.at[k, j, z, x]
                send_if(above, block, block, cz_send.at[0], line_recv.at[k, j, z], {"kv": (z + 1) * nx + x})
                send_if(below, block, block, cz_send.at[1], line_recv.at[k, j, z - 1], {"kv": (z - 1) * nx + x})
                across(block, cx_send.at[0], side_recv.at[k, z])

    room = jnp.minimum(z, nz - 1 - z)

    def near(s):
        step = jnp.where(s <= 2 * room, (s + 1) // 2, s - room)
        up = jnp.where(s <= 2 * room, s % 2 == 1, z < nz - 1 - z)
        return jnp.where(up, z + step, z - step)

    order = [z] + [near(s) for s in range(1, nz)]

    def forward(k, s):
        g = order[s]
        up = g < z
        onward = jnp.where(up, z < nz - 1, z > 0)
        device = {"kv": jnp.where(up, z + 1, z - 1) * nx + x}
        place = jnp.where(up, g, g - 1)
        for j in range(PIECES):
            block, recv = mid.at[k, j, g, x], line_recv.at[k, j, place]
            arrive(block, recv)
            send_if(onward, block, block, cz_send.at[1 + s], recv, device)
            across(block, cx_send.at[1], side_recv.at[k, g])

    def drain_gather():
        sent(mid.at[:, :, 0, 0:nx - 1], cx_send.at[0])
        sent(mid.at[:, :, 0:nz - 1, 0:nx - 1], cx_send.at[1])
        straight = mid.at[:, :, 0, 0]
        pl.when(above)(functools.partial(sent, straight, cz_send.at[0]))
        pl.when(below)(functools.partial(sent, straight, cz_send.at[1]))
        for s in range(1, nz):
            onward = jnp.where(order[s] < z, z < nz - 1, z > 0)
            pl.when(onward)(functools.partial(sent, straight, cz_send.at[1 + s]))

    inverse = finish(0, False)
    for k in range(parts):
        for h in range(heads):
            retain(k, h)
            if h == 0 and k + 1 < parts:
                for d in range(1, ny):
                    relay(k + 1, d)
        output(k, inverse)
        if k + 1 < parts:
            inverse = finish(k + 1, True)
            pairs(k)
    if parts > 1:
        launch(0)
    pairs(parts - 1)
    gain2[...] = chan_gain[...].astype(F32).reshape(1, width)
    if parts > 1:
        forward(0, 1)
        pl.when(room > 0)(functools.partial(forward, 0, 2))
    launch(parts - 1)
    if parts > 1:
        pl.when(room == 0)(functools.partial(forward, 0, 2))
    for k in range(parts):
        for s in range(1 if k or parts == 1 else 3, nz):
            forward(k, s)
    sent(xf.at[0:2 * ny - 1], a_send.at[0])
    sent(r1, b1_send.at[0])
    sent(s2, b2_send.at[0])

    tall = nx * few
    total_rows = nz * tall
    hidden_units = wu.shape[1]
    up_tile = min(256, hidden_units)
    down_tile = min(256, strip)

    def gather(k):
        for s in range(nz):
            g = order[s]
            at = pl.ds(pl.multiple_of(g * tall, tall), tall)
            for d in range(1, nx):
                arrive(mid.at[k, :, g, xs(d)], side_recv.at[k, g, d - 1])
            for j in range(PIECES):
                wide = mid[k, j, g].reshape(tall, piece).astype(F32)
                lhs[at, j * piece:(j + 1) * piece] = (wide * gain2[:, j * piece:(j + 1) * piece]).astype(BF16)
        sums = jnp.zeros((total_rows, 1), F32)
        for j in range(PIECES):
            wide = mid[k, j].reshape(total_rows, piece).astype(F32)
            sums += jnp.sum(wide * wide, axis=1, keepdims=True)
        return lax.rsqrt(sums * (1.0 / width) + EPSILON)

    def mixer(k):
        rms = gather(k)
        if k == 0:
            wu_load.wait()

        @pl.loop(0, hidden_units // up_tile)
        def _(i):
            at = pl.ds(pl.multiple_of(i * up_tile, up_tile), up_tile)
            hidden = jnp.maximum(dot(lhs[...], wu[:, at]) * rms, 0.0)
            act[:, at] = (hidden * hidden).astype(BF16)

        if k == 0:
            wd_load.wait()

        for q in range(SLICES):
            for i in range(strip // down_tile):
                low = q * strip + i * down_tile
                down = dot(act[...], wd[:, low:low + down_tile]).astype(BF16)
                for zz in range(nz):
                    for xx in range(nx):
                        first = (zz * nx + xx) * few
                        sx[k, xx, zz, q, :, i * down_tile:(i + 1) * down_tile] = down[first:first + few]
            if q % per_wave == per_wave - 1:
                swap(k, nz - 1, q // per_wave)
                if k > 0:
                    reduce_x(k - 1, nz - 1, q // per_wave)
        for s in range(nz - 2, 0, -1):
            for p in range(WAVES):
                swap(k, s, p)

    per_wave = SLICES // WAVES

    def wave(p):
        return slice(p * per_wave, (p + 1) * per_wave)

    def swap(k, s, p):
        g = order[s]
        for d in range(1, nx):
            send(
                sx.at[k, xs(d), g, wave(p)], rx.at[k, nx - 1 - d, g, wave(p)],
                dx_send.at[0], dx_recv.at[k, s - 1, p], {"kv": z * nx + xs(d)},
            )

    def reduce_x(k, s, p):
        g = order[s]
        arrive(rx.at[k, :, g, wave(p)], dx_recv.at[k, s - 1, p])
        total = sx[k, x, g, wave(p)].astype(F32)
        for d in range(1, nx):
            total += rx[k, d - 1, g, wave(p)].astype(F32)
        sz[k, g, wave(p)] = total.astype(BF16)
        send(sz.at[k, g, wave(p)], rz.at[k, z, wave(p)], dz_send.at[0], dz_recv.at[k, p], {"kv": g * nx + x})

    for k in range(parts):
        mixer(k)
    for k in range(parts):
        for d in range(1, nx):
            send(sx.at[k, xs(d), z], own.at[k, nx - 1 - d], dx_send.at[1], own_recv.at[k], {"kv": z * nx + xs(d)})
    for k in range(parts):
        for s in range(nz - 1, 0, -1):
            if k == parts - 1 or s < nz - 1:
                for p in range(WAVES):
                    reduce_x(k, s, p)
    drain_gather()

    per_strip = strip // feats
    per_piece = piece // strip if piece > strip else 1
    for k in range(parts):
        arrive(own.at[k], own_recv.at[k])
        for q in range(SLICES):
            inside = q % per_piece
            total = sx[k, x, z, q].astype(F32)
            for d in range(1, nx):
                total += own[k, d - 1, q].astype(F32)
            total += mid[k, q // per_piece, z, x, :, inside * strip:(inside + 1) * strip].astype(F32)
            if q % per_wave == 0:
                arrive(rz.at[k, 0:nz - 1, 0:per_wave], dz_recv.at[k, q // per_wave])
            for s in range(1, nz):
                total += rz[k, order[s], q].astype(F32)
            done = total.astype(BF16)
            for i in range(per_strip):
                t = q * per_strip + i
                fin[k, t] = done[:, i * feats:(i + 1) * feats]

                @pl.when(tp != t)
                def _(t=t, k=k):
                    make(fin.at[k, t], ob.at[k, tp], e_send.at[0], e_recv.at[k], {"tp": t}).start()

                @pl.when(tp == t)
                def _(t=t, k=k):
                    ob[k, tp] = fin[k, t]

    sent(rx.at[:, :, 0:nz - 1], dx_send.at[0])
    sent(own, dx_send.at[1])
    sent(sz.at[:, 0:nz - 1], dz_send.at[0])
    for k in range(parts):
        arrive(ob.at[k, 0:n_tp - 1], e_recv.at[k])
    sent(ob.at[:, 0:n_tp - 1], e_send.at[0])
    out_ref[...] = ob[...].reshape(rows, feats)


def publish(out_ref, st, out_hbm, st_hbm, sem):
    heads, head = st.shape[0], st.shape[1]
    cuts = 2
    copies = []
    for h in range(heads):
        for i in range(cuts):
            at = pl.ds(i * (head // cuts), head // cuts)
            copies.append(pltpu.make_async_copy(st.at[h, at], st_hbm.at[h, at], sem.at[1 + h * cuts + i]))
    copies.append(pltpu.make_async_copy(out_ref, out_hbm, sem.at[0]))
    for copy in copies:
        copy.start()
    for copy in copies:
        copy.wait()


def local(
    n_kv, n_tp,
    tokens, states, mix_gain, w_query, w_key, w_value, w_gate, head_gain, w_output,
    channel_gain, w_up, w_down,
):
    rows, feats = tokens.shape
    heads, head = states.shape[1], states.shape[2]
    width = mix_gain.shape[0]
    inner = w_query.shape[1]
    hidden = w_up.shape[1]
    share = rows // n_tp
    nx = 1
    while (2 * nx) ** 2 <= n_kv:
        nx *= 2
    nz = n_kv // nx
    ny = n_tp // CORES
    cut = width // CUTS
    piece = width // PIECES
    strip = width // SLICES
    parts = 2 if share % 32 == 0 else 1
    few = share // parts
    angles = POS * ROTARY_BASE ** (-np.arange(head // 2) / (head // 2))
    turn = np.concatenate([np.cos(angles), np.sin(angles)])[:, None]
    turn = jnp.asarray(np.broadcast_to(turn, (head, rows)), F32)
    sizes = (n_tp, ny, nz, nx, heads, head, rows, feats, share, width, parts)
    hbm = pl.BlockSpec(memory_space=pltpu.HBM)
    vmem = pl.BlockSpec(memory_space=pltpu.VMEM)
    dma = pltpu.SemaphoreType.DMA
    layer_out, new_states = pl.pallas_call(
        functools.partial(kernel, sizes),
        out_shape=(
            pltpu.VMEM((rows, feats), BF16),
            pltpu.VMEM((heads, head, head, rows), F32),
        ),
        in_specs=[hbm] * 13,
        out_specs=(vmem, vmem),
        scratch_shapes=[
            pltpu.VMEM((width,), BF16),
            pltpu.VMEM((width,), BF16),
            pltpu.VMEM((inner,), BF16),
            pltpu.VMEM((head, rows), F32),
            pltpu.VMEM((1, width), F32),
            pltpu.VMEM((1, width), F32),
            pltpu.VMEM((n_tp, rows, feats), BF16),
            pltpu.VMEM((4, width, inner), BF16),
            pltpu.VMEM((inner, width), BF16),
            pltpu.VMEM((width, hidden), BF16),
            pltpu.VMEM((hidden, width), BF16),
            pltpu.VMEM((4, rows, inner), F32),
            pltpu.VMEM((inner, rows), F32),
            pltpu.VMEM((inner, rows), F32),
            pltpu.VMEM((inner, rows), F32),
            pltpu.VMEM((inner, rows), F32),
            pltpu.VMEM((parts, CUTS, CORES, ny, few, cut), BF16),
            pltpu.VMEM((parts, CUTS, ny, few, cut), BF16),
            pltpu.VMEM((parts, CUTS, ny - 1, few, cut), BF16),
            pltpu.VMEM((parts, CUTS, ny - 1, few, cut), BF16),
            pltpu.VMEM((parts, PIECES, nz, nx, few, piece), BF16),
            pltpu.VMEM((nz * nx * few, width), BF16),
            pltpu.VMEM((nz * nx * few, hidden), BF16),
            pltpu.VMEM((parts, nx, nz, SLICES, few, strip), BF16),
            pltpu.VMEM((parts, nx - 1, nz, SLICES, few, strip), BF16),
            pltpu.VMEM((parts, nx - 1, SLICES, few, strip), BF16),
            pltpu.VMEM((parts, nz, SLICES, few, strip), BF16),
            pltpu.VMEM((parts, nz, SLICES, few, strip), BF16),
            pltpu.VMEM((parts, n_tp, few, feats), BF16),
            pltpu.VMEM((parts, n_tp, few, feats), BF16),
            dma((7,)),
            dma((1,)),
            dma((parts, n_tp)),
            dma((1,)),
            dma((parts, CUTS)),
            dma((1,)),
            dma((parts, CUTS, ny - 1)),
            dma((2,)),
            dma((1 + nz,)),
            dma((parts, PIECES, nz - 1)),
            dma((parts, nz, nx - 1)),
            dma((2,)),
            dma((parts, nz - 1, WAVES)),
            dma((parts,)),
            dma((1,)),
            dma((parts, WAVES)),
            dma((1,)),
            dma((parts,)),
        ],
        compiler_params=pltpu.CompilerParams(
            collective_id=0, has_side_effects=True, vmem_limit_bytes=48 * 1024 * 1024
        ),
    )(
        tokens, jnp.transpose(states, (1, 2, 3, 0)), mix_gain, w_query, w_key, w_value,
        w_gate, head_gain, w_output, channel_gain, w_up, w_down, turn,
    )
    layer_out, new_states = pl.pallas_call(
        publish,
        out_shape=(
            jax.ShapeDtypeStruct((rows, feats), BF16),
            jax.ShapeDtypeStruct((heads, head, head, rows), F32),
        ),
        in_specs=[vmem, vmem],
        out_specs=(hbm, hbm),
        scratch_shapes=[dma((1 + 2 * heads,))],
        compiler_params=pltpu.CompilerParams(vmem_limit_bytes=1024 * 1024),
    )(
        pltpu.with_memory_space_constraint(layer_out, pltpu.VMEM),
        pltpu.with_memory_space_constraint(new_states, pltpu.VMEM),
    )
    return (layer_out, jnp.transpose(new_states, (3, 0, 1, 2)))


def solution(mesh):
    placed = (
        P("kv", "tp"),
        P("kv", "tp", None, None),
        P(),
        P(None, "tp"),
        P(None, "tp"),
        P(None, "tp"),
        P(None, "tp"),
        P("tp"),
        P("tp", None),
        P(),
        P(None, "kv"),
        P("kv", None),
    )
    return jax.shard_map(
        functools.partial(local, mesh.shape["kv"], mesh.shape["tp"]),
        mesh=mesh,
        in_specs=placed,
        out_specs=(P("kv", "tp"), P("kv", "tp", None, None)),
        check_vma=False,
    )
```

```python
import functools

import jax
import jax.numpy as jnp
import numpy as np
from jax import lax
from jax.experimental import pallas as pl
from jax.experimental.pallas import tpu as pltpu
from jax.sharding import PartitionSpec as P

POS = 16384
EPSILON = 1e-06
ROTARY_BASE = 10000.0
CORES = 2
CUTS = 2
PIECES = 4
SLICES = 4
WAVES = 2
MESH = pl.DeviceIdType.MESH
F32 = jnp.float32
BF16 = jnp.bfloat16


def dot(a, b):
    return jnp.dot(a, b, preferred_element_type=F32)


def kernel(
    sizes,
    tok_hbm, st_hbm, mix_hbm, wq_hbm, wk_hbm, wv_hbm, wg_hbm, head_hbm, wo_hbm,
    chan_hbm, wu_hbm, wd_hbm, turn_hbm,
    out_ref, st,
    mix_gain, chan_gain, head_gain, turn, gain1, gain2,
    xf, wproj, wo, wu, wd, acc, qt, kt, vt, rt,
    part, r1, s2, r2, mid, lhs, act, sx, rx, own, sz, rz, fin, ob,
    load_sem, a_send, a_recv, b1_send, b1_recv, b2_send, b2_recv,
    cx_send, cz_send, line_recv, side_recv,
    dx_send, dx_recv, own_recv, dz_send, dz_recv, e_send, e_recv,
):
    n_tp, ny, nz, nx, heads, head, rows, feats, share, width, parts = sizes
    tp = lax.axis_index("tp")
    kv = lax.axis_index("kv")
    c, y = lax.rem(tp, CORES), tp // CORES
    x, z = lax.rem(kv, nx), kv // nx
    other = 1 - c
    partner = y * CORES + other
    half = head // 2
    cut = width // CUTS
    piece = width // PIECES
    strip = width // SLICES
    few = share // parts

    def ys(d):
        return lax.rem(y + d, ny)

    def zs(d):
        return lax.rem(z + d, nz)

    def xs(d):
        return lax.rem(x + d, nx)

    def make(src, dst, ssem, rsem, device):
        return pltpu.make_async_remote_copy(
            src_ref=src, dst_ref=dst, send_sem=ssem, recv_sem=rsem,
            device_id=device, device_id_type=MESH,
        )

    def send(src, dst, ssem, rsem, device):
        make(src, dst, ssem, rsem, device).start()

    def send_if(cond, src, dst, ssem, rsem, device):
        pl.when(cond)(make(src, dst, ssem, rsem, device).start)

    def arrive(dst, rsem):
        make(dst, dst, a_send.at[0], rsem, {"tp": partner}).wait_recv()

    def sent(src, ssem):
        make(src, src, ssem, a_recv.at[0, 0], {"tp": partner}).wait_send()

    barrier = pltpu.get_barrier_semaphore()
    greeted = 0
    for d in range(1, n_tp):
        pl.semaphore_signal(barrier, inc=1, device_id={"tp": lax.rem(tp + d, n_tp)}, device_id_type=MESH)
        greeted += 1
    for d in range(1, nx):
        pl.semaphore_signal(barrier, inc=1, device_id={"kv": z * nx + xs(d)}, device_id_type=MESH)
        greeted += 1
    for d in range(1, nz):
        pl.semaphore_signal(barrier, inc=1, device_id={"kv": zs(d) * nx + x}, device_id_type=MESH)
        greeted += 1

    slots = iter(range(7))

    def load(src, dst, slot=None):
        copy = pltpu.make_async_copy(src, dst, load_sem.at[next(slots) if slot is None else slot])
        copy.start()
        return copy

    tok_load = load(tok_hbm, xf.at[tp])
    small, shared, state = next(slots), next(slots), next(slots)
    load(mix_hbm, mix_gain, small)
    load(turn_hbm, turn, small)
    load(head_hbm, head_gain, small)
    load(chan_hbm, chan_gain, small)
    for i, w in enumerate((wq_hbm, wk_hbm, wv_hbm, wg_hbm)):
        load(w, wproj.at[i], shared)
    for h in range(heads):
        load(st_hbm.at[h], st.at[h], state)
    wo_load = load(wo_hbm, wo)
    wu_load = load(wu_hbm, wu)
    wd_load = load(wd_hbm, wd)
    tok_load.wait()
    pl.semaphore_wait(barrier, greeted)

    band = rows // parts

    def cutout(slot, k):
        return xf.at[slot, k * band:(k + 1) * band]

    for k in range(parts):
        for d in range(1, ny):
            send(cutout(tp, k), cutout(tp, k), a_send.at[0], a_recv.at[k, tp], {"tp": ys(d) * CORES + c})
        send(cutout(tp, k), cutout(tp, k), a_send.at[0], a_recv.at[k, tp], {"tp": partner})
    for ref in (mix_gain, turn, head_gain, chan_gain):
        pltpu.make_async_copy(ref, ref, load_sem.at[small]).wait()
    gain1[...] = mix_gain[...].astype(F32).reshape(1, width)
    pltpu.make_async_copy(wproj, wproj, load_sem.at[shared]).wait()

    def project(slot, low, count, first):
        at = pl.ds(pl.multiple_of(slot * feats, feats), feats)
        wide = xf[slot, low:low + count].astype(F32)
        scaled = (wide * gain1[:, at]).astype(BF16)
        for i in range(4):
            term = dot(scaled, wproj[i, at, :])
            if first:
                acc[i, low:low + count] = term
            else:
                acc[i, low:low + count] += term
        return jnp.sum(wide * wide, axis=1, keepdims=True)

    near_squares = project(tp, 0, rows, True)
    for k in range(parts):
        arrive(cutout(partner, k), a_recv.at[k, partner])
    near_squares += project(partner, 0, rows, False)

    def relay(k, d):
        slot = ys(d) * CORES + c
        arrive(cutout(slot, k), a_recv.at[k, slot])
        send(cutout(slot, k), cutout(slot, k), a_send.at[0], a_recv.at[k, slot], {"tp": partner})

    def finish(k, relayed):
        low = k * band
        squares = near_squares[low:low + band]
        for d in range(1, ny):
            if not relayed:
                relay(k, d)
            squares += project(ys(d) * CORES + c, low, band, False)
            slot = ys(d) * CORES + other
            arrive(cutout(slot, k), a_recv.at[k, slot])
            squares += project(slot, low, band, False)
        inverse = lax.rsqrt(squares * (1.0 / width) + EPSILON)

        def columns(i):
            value = acc[i, low:low + band] * inverse
            lead = [jnp.zeros((low, value.shape[1]), F32)] if low else []
            rest = [jnp.zeros((rows - low - band, value.shape[1]), F32)] if low + band < rows else []
            return jnp.concatenate(lead + [value] + rest, axis=0).T

        qt[...] = columns(0)
        kt[...] = columns(1)
        vt[...] = columns(2)
        cosine, sine = turn[:half, :], turn[half:, :]
        for h in range(heads):
            lo, hi = pl.ds(h * head, half), pl.ds(h * head + half, half)
            for ref, scale in ((qt, head ** -0.5), (kt, 1.0)):
                a, b = ref[lo, :], ref[hi, :]
                ref[lo, :] = (a * cosine - b * sine) * scale
                ref[hi, :] = (a * sine + b * cosine) * scale
        return inverse

    def retain(k, h):
        if k == 0 and h == 0:
            pltpu.make_async_copy(st, st, load_sem.at[state]).wait()
        number = (tp * heads + h).astype(F32)
        decay = 1.0 - jnp.exp2(-1.0 - 11.0 * jnp.full((1, rows), number, F32) / (heads * n_tp - 1))
        lane = lax.broadcasted_iota(jnp.int32, (1, rows), 1)
        decay = jnp.where((lane >= k * band) & (lane < (k + 1) * band), decay, 1.0)
        value = vt[pl.ds(h * head, head), :]
        base = h * head

        def step(i, total):
            fresh = decay * st[h, i] + kt[pl.ds(base + i, 1), :] * value
            st[h, i] = fresh
            return total + qt[pl.ds(base + i, 1), :] * fresh

        total = lax.fori_loop(0, head, step, jnp.zeros((head, rows), F32), unroll=8)
        center = total - jnp.mean(total, axis=0, keepdims=True)
        spread = jnp.mean(center * center, axis=0, keepdims=True)
        rt[pl.ds(base, head), :] = center * lax.rsqrt(spread + EPSILON)

    def output(k, inverse):
        low = k * band
        gating = acc[3, low:low + band] * inverse
        if k == 0:
            wo_load.wait()
        normal = rt[...].T[low:low + band]
        gated = (normal * head_gain[...].astype(F32).reshape(1, heads * head) * (gating * jax.nn.sigmoid(gating))).astype(BF16)
        for j in range(CUTS):
            whole = dot(gated, wo[:, j * cut:(j + 1) * cut]).astype(BF16)
            for t in range(n_tp):
                part[k, j, t % CORES, t // CORES] = whole[t * few:(t + 1) * few]
            send(part.at[k, j, other], r1.at[k, j], b1_send.at[0], b1_recv.at[k, j], {"tp": partner})

    def pairs(k):
        for j in range(CUTS):
            arrive(r1.at[k, j], b1_recv.at[k, j])
            for d in range(1, ny):
                to = ys(d)
                s2[k, j, d - 1] = (part[k, j, c, to].astype(F32) + r1[k, j, to].astype(F32)).astype(BF16)
                send(s2.at[k, j, d - 1], r2.at[k, j, d - 1], b2_send.at[0], b2_recv.at[k, j, d - 1], {"tp": to * CORES + c})

    below, above = z > 0, z < nz - 1
    leap = nz == 4 and parts > 1
    room = jnp.minimum(z, nz - 1 - z)

    def across(block, sem, recv):
        for d in range(1, nx):
            send(block, block, sem, recv.at[nx - 1 - d], {"kv": z * nx + xs(d)})

    def launch(k):
        own_rows = pl.ds(pl.multiple_of(k * band + tp * few, few), few)
        for b in range(CUTS):
            total = part[k, b, c, y].astype(F32) + r1[k, b, y].astype(F32)
            for d in range(1, ny):
                arrive(r2.at[k, b, d - 1], b2_recv.at[k, b, d - 1])
                total += r2[k, b, d - 1].astype(F32)
            per = n_tp // CUTS
            mine = jnp.concatenate([xf[t, own_rows, :] for t in range(b * per, (b + 1) * per)], axis=1)
            middle = (mine.astype(F32) + total).astype(BF16)
            for i in range(cut // piece):
                j = b * (cut // piece) + i
                mid[k, j, z, x] = middle[:, i * piece:(i + 1) * piece]
                block = mid.at[k, j, z, x]
                send_if(above, block, block, cz_send.at[0], line_recv.at[k, j, z], {"kv": (z + 1) * nx + x})
                send_if(below, block, block, cz_send.at[1], line_recv.at[k, j, z - 1], {"kv": (z - 1) * nx + x})
                if leap:
                    far = nz - 1 - z
                    place = jnp.where(above, z, z - 1)
                    send_if(room == 0, block, block, cz_send.at[nz], line_recv.at[k, j, place], {"kv": far * nx + x})
                across(block, cx_send.at[0], side_recv.at[k, z])

    def near(s):
        step = jnp.where(s <= 2 * room, (s + 1) // 2, s - room)
        up = jnp.where(s <= 2 * room, s % 2 == 1, z < nz - 1 - z)
        return jnp.where(up, z + step, z - step)

    order = [z] + [near(s) for s in range(1, nz)]

    def forward(k, s):
        g = order[s]
        up = g < z
        onward = jnp.where(up, z < nz - 1, z > 0)
        device = {"kv": jnp.where(up, z + 1, z - 1) * nx + x}
        place = jnp.where(up, g, g - 1)
        for j in range(PIECES):
            block, recv = mid.at[k, j, g, x], line_recv.at[k, j, place]
            arrive(block, recv)
            if not (leap and s == nz - 1):
                send_if(onward, block, block, cz_send.at[1 + s], recv, device)
            across(block, cx_send.at[1], side_recv.at[k, g])

    def drain_gather():
        sent(mid.at[:, :, 0, 0:nx - 1], cx_send.at[0])
        sent(mid.at[:, :, 0:nz - 1, 0:nx - 1], cx_send.at[1])
        straight = mid.at[:, :, 0, 0]
        pl.when(above)(functools.partial(sent, straight, cz_send.at[0]))
        pl.when(below)(functools.partial(sent, straight, cz_send.at[1]))
        for s in range(1, nz):
            onward = jnp.where(order[s] < z, z < nz - 1, z > 0)
            if leap and s == nz - 1:
                onward = room == 0
            pl.when(onward)(functools.partial(sent, straight, cz_send.at[1 + s]))

    inverse = finish(0, False)
    for k in range(parts):
        for h in range(heads):
            retain(k, h)
            if h == 0 and k + 1 < parts:
                for d in range(1, ny):
                    relay(k + 1, d)
        output(k, inverse)
        if k + 1 < parts:
            inverse = finish(k + 1, True)
            pairs(k)
    if parts > 1:
        launch(0)
    pairs(parts - 1)
    gain2[...] = chan_gain[...].astype(F32).reshape(1, width)
    if parts > 1:
        forward(0, 1)
        pl.when(room > 0)(functools.partial(forward, 0, 2))
    launch(parts - 1)
    if parts > 1:
        pl.when(room == 0)(functools.partial(forward, 0, 2))
    if leap:
        forward(0, 3)
        forward(1, 1)
        pl.when(room > 0)(functools.partial(forward, 1, 2))
    else:
        for k in range(parts):
            for s in range(1 if k or parts == 1 else 3, nz):
                forward(k, s)
    sent(xf.at[0:2 * ny - 1], a_send.at[0])
    sent(r1, b1_send.at[0])
    sent(s2, b2_send.at[0])

    tall = nx * few
    total_rows = nz * tall
    hidden_units = wu.shape[1]
    up_tile = min(256, hidden_units)
    down_tile = min(256, strip)

    def gather(k):
        for s in range(nz):
            g = order[s]
            at = pl.ds(pl.multiple_of(g * tall, tall), tall)
            for d in range(1, nx):
                arrive(mid.at[k, :, g, xs(d)], side_recv.at[k, g, d - 1])
            for j in range(PIECES):
                wide = mid[k, j, g].reshape(tall, piece).astype(F32)
                lhs[at, j * piece:(j + 1) * piece] = (wide * gain2[:, j * piece:(j + 1) * piece]).astype(BF16)
        sums = jnp.zeros((total_rows, 1), F32)
        for j in range(PIECES):
            wide = mid[k, j].reshape(total_rows, piece).astype(F32)
            sums += jnp.sum(wide * wide, axis=1, keepdims=True)
        return lax.rsqrt(sums * (1.0 / width) + EPSILON)

    def mixer(k):
        rms = gather(k)
        if k == 0:
            wu_load.wait()

        @pl.loop(0, hidden_units // up_tile)
        def _(i):
            at = pl.ds(pl.multiple_of(i * up_tile, up_tile), up_tile)
            hidden = jnp.maximum(dot(lhs[...], wu[:, at]) * rms, 0.0)
            act[:, at] = (hidden * hidden).astype(BF16)

        if k == 0:
            wd_load.wait()
            if leap:
                forward(1, 3)
                pl.when(room == 0)(functools.partial(forward, 1, 2))

        for q in range(SLICES):
            for i in range(strip // down_tile):
                low = q * strip + i * down_tile
                down = dot(act[...], wd[:, low:low + down_tile]).astype(BF16)
                for zz in range(nz):
                    for xx in range(nx):
                        first = (zz * nx + xx) * few
                        sx[k, xx, zz, q, :, i * down_tile:(i + 1) * down_tile] = down[first:first + few]
            if q % per_wave == per_wave - 1:
                swap(k, nz - 1, q // per_wave)
                if k > 0:
                    reduce_x(k - 1, nz - 1, q // per_wave)
        for s in range(nz - 2, 0, -1):
            for p in range(WAVES):
                swap(k, s, p)

    per_wave = SLICES // WAVES

    def wave(p):
        return slice(p * per_wave, (p + 1) * per_wave)

    def swap(k, s, p):
        g = order[s]
        for d in range(1, nx):
            send(
                sx.at[k, xs(d), g, wave(p)], rx.at[k, nx - 1 - d, g, wave(p)],
                dx_send.at[0], dx_recv.at[k, s - 1, p], {"kv": z * nx + xs(d)},
            )

    def reduce_x(k, s, p):
        g = order[s]
        arrive(rx.at[k, :, g, wave(p)], dx_recv.at[k, s - 1, p])
        total = sx[k, x, g, wave(p)].astype(F32)
        for d in range(1, nx):
            total += rx[k, d - 1, g, wave(p)].astype(F32)
        sz[k, g, wave(p)] = total.astype(BF16)
        send(sz.at[k, g, wave(p)], rz.at[k, z, wave(p)], dz_send.at[0], dz_recv.at[k, p], {"kv": g * nx + x})

    for k in range(parts):
        mixer(k)
    for k in range(parts):
        for d in range(1, nx):
            send(sx.at[k, xs(d), z], own.at[k, nx - 1 - d], dx_send.at[1], own_recv.at[k], {"kv": z * nx + xs(d)})
    for k in range(parts):
        for s in range(nz - 1, 0, -1):
            if k == parts - 1 or s < nz - 1:
                for p in range(WAVES):
                    reduce_x(k, s, p)
    drain_gather()

    per_strip = strip // feats
    per_piece = piece // strip if piece > strip else 1
    for k in range(parts):
        arrive(own.at[k], own_recv.at[k])
        for q in range(SLICES):
            inside = q % per_piece
            total = sx[k, x, z, q].astype(F32)
            for d in range(1, nx):
                total += own[k, d - 1, q].astype(F32)
            total += mid[k, q // per_piece, z, x, :, inside * strip:(inside + 1) * strip].astype(F32)
            if q % per_wave == 0:
                arrive(rz.at[k, 0:nz - 1, 0:per_wave], dz_recv.at[k, q // per_wave])
            for s in range(1, nz):
                total += rz[k, order[s], q].astype(F32)
            done = total.astype(BF16)
            for i in range(per_strip):
                t = q * per_strip + i
                fin[k, t] = done[:, i * feats:(i + 1) * feats]

                @pl.when(tp != t)
                def _(t=t, k=k):
                    make(fin.at[k, t], ob.at[k, tp], e_send.at[0], e_recv.at[k], {"tp": t}).start()

                @pl.when(tp == t)
                def _(t=t, k=k):
                    ob[k, tp] = fin[k, t]

    sent(rx.at[:, :, 0:nz - 1], dx_send.at[0])
    sent(own, dx_send.at[1])
    sent(sz.at[:, 0:nz - 1], dz_send.at[0])
    for k in range(parts):
        arrive(ob.at[k, 0:n_tp - 1], e_recv.at[k])
    sent(ob.at[:, 0:n_tp - 1], e_send.at[0])
    out_ref[...] = ob[...].reshape(rows, feats)


def publish(out_ref, st, out_hbm, st_hbm, sem):
    heads, head = st.shape[0], st.shape[1]
    cuts = 2
    copies = []
    for h in range(heads):
        for i in range(cuts):
            at = pl.ds(i * (head // cuts), head // cuts)
            copies.append(pltpu.make_async_copy(st.at[h, at], st_hbm.at[h, at], sem.at[1 + h * cuts + i]))
    copies.append(pltpu.make_async_copy(out_ref, out_hbm, sem.at[0]))
    for copy in copies:
        copy.start()
    for copy in copies:
        copy.wait()


def local(
    n_kv, n_tp,
    tokens, states, mix_gain, w_query, w_key, w_value, w_gate, head_gain, w_output,
    channel_gain, w_up, w_down,
):
    rows, feats = tokens.shape
    heads, head = states.shape[1], states.shape[2]
    width = mix_gain.shape[0]
    inner = w_query.shape[1]
    hidden = w_up.shape[1]
    share = rows // n_tp
    nx = 1
    while (2 * nx) ** 2 <= n_kv:
        nx *= 2
    nz = n_kv // nx
    ny = n_tp // CORES
    cut = width // CUTS
    piece = width // PIECES
    strip = width // SLICES
    parts = 2 if share % 32 == 0 else 1
    few = share // parts
    angles = POS * ROTARY_BASE ** (-np.arange(head // 2) / (head // 2))
    turn = np.concatenate([np.cos(angles), np.sin(angles)])[:, None]
    turn = jnp.asarray(np.broadcast_to(turn, (head, rows)), F32)
    sizes = (n_tp, ny, nz, nx, heads, head, rows, feats, share, width, parts)
    hbm = pl.BlockSpec(memory_space=pltpu.HBM)
    vmem = pl.BlockSpec(memory_space=pltpu.VMEM)
    dma = pltpu.SemaphoreType.DMA
    layer_out, new_states = pl.pallas_call(
        functools.partial(kernel, sizes),
        out_shape=(
            pltpu.VMEM((rows, feats), BF16),
            pltpu.VMEM((heads, head, head, rows), F32),
        ),
        in_specs=[hbm] * 13,
        out_specs=(vmem, vmem),
        scratch_shapes=[
            pltpu.VMEM((width,), BF16),
            pltpu.VMEM((width,), BF16),
            pltpu.VMEM((inner,), BF16),
            pltpu.VMEM((head, rows), F32),
            pltpu.VMEM((1, width), F32),
            pltpu.VMEM((1, width), F32),
            pltpu.VMEM((n_tp, rows, feats), BF16),
            pltpu.VMEM((4, width, inner), BF16),
            pltpu.VMEM((inner, width), BF16),
            pltpu.VMEM((width, hidden), BF16),
            pltpu.VMEM((hidden, width), BF16),
            pltpu.VMEM((4, rows, inner), F32),
            pltpu.VMEM((inner, rows), F32),
            pltpu.VMEM((inner, rows), F32),
            pltpu.VMEM((inner, rows), F32),
            pltpu.VMEM((inner, rows), F32),
            pltpu.VMEM((parts, CUTS, CORES, ny, few, cut), BF16),
            pltpu.VMEM((parts, CUTS, ny, few, cut), BF16),
            pltpu.VMEM((parts, CUTS, ny - 1, few, cut), BF16),
            pltpu.VMEM((parts, CUTS, ny - 1, few, cut), BF16),
            pltpu.VMEM((parts, PIECES, nz, nx, few, piece), BF16),
            pltpu.VMEM((nz * nx * few, width), BF16),
            pltpu.VMEM((nz * nx * few, hidden), BF16),
            pltpu.VMEM((parts, nx, nz, SLICES, few, strip), BF16),
            pltpu.VMEM((parts, nx - 1, nz, SLICES, few, strip), BF16),
            pltpu.VMEM((parts, nx - 1, SLICES, few, strip), BF16),
            pltpu.VMEM((parts, nz, SLICES, few, strip), BF16),
            pltpu.VMEM((parts, nz, SLICES, few, strip), BF16),
            pltpu.VMEM((parts, n_tp, few, feats), BF16),
            pltpu.VMEM((parts, n_tp, few, feats), BF16),
            dma((7,)),
            dma((1,)),
            dma((parts, n_tp)),
            dma((1,)),
            dma((parts, CUTS)),
            dma((1,)),
            dma((parts, CUTS, ny - 1)),
            dma((2,)),
            dma((1 + nz,)),
            dma((parts, PIECES, nz - 1)),
            dma((parts, nz, nx - 1)),
            dma((2,)),
            dma((parts, nz - 1, WAVES)),
            dma((parts,)),
            dma((1,)),
            dma((parts, WAVES)),
            dma((1,)),
            dma((parts,)),
        ],
        compiler_params=pltpu.CompilerParams(
            collective_id=0, has_side_effects=True, vmem_limit_bytes=48 * 1024 * 1024
        ),
    )(
        tokens, jnp.transpose(states, (1, 2, 3, 0)), mix_gain, w_query, w_key, w_value,
        w_gate, head_gain, w_output, channel_gain, w_up, w_down, turn,
    )
    layer_out, new_states = pl.pallas_call(
        publish,
        out_shape=(
            jax.ShapeDtypeStruct((rows, feats), BF16),
            jax.ShapeDtypeStruct((heads, head, head, rows), F32),
        ),
        in_specs=[vmem, vmem],
        out_specs=(hbm, hbm),
        scratch_shapes=[dma((1 + 2 * heads,))],
        compiler_params=pltpu.CompilerParams(vmem_limit_bytes=1024 * 1024),
    )(
        pltpu.with_memory_space_constraint(layer_out, pltpu.VMEM),
        pltpu.with_memory_space_constraint(new_states, pltpu.VMEM),
    )
    return (layer_out, jnp.transpose(new_states, (3, 0, 1, 2)))


def solution(mesh):
    placed = (
        P("kv", "tp"),
        P("kv", "tp", None, None),
        P(),
        P(None, "tp"),
        P(None, "tp"),
        P(None, "tp"),
        P(None, "tp"),
        P("tp"),
        P("tp", None),
        P(),
        P(None, "kv"),
        P("kv", None),
    )
    return jax.shard_map(
        functools.partial(local, mesh.shape["kv"], mesh.shape["tp"]),
        mesh=mesh,
        in_specs=placed,
        out_specs=(P("kv", "tp"), P("kv", "tp", None, None)),
        check_vma=False,
    )
```
